32 devices in a mesh: sp: 8 (over z, x), dp: 4 (over y, core).
Axes of the slice: x: 2, y: 2, z: 4, core: 2. Of those that a mesh axis runs over, the one named last changes fastest.
Arguments:
- queries: bfloat16 [4, 1024, 16, 128], P('dp', 'sp'), may hold values from -6 to 6
- key_rows: bfloat16 [4, 1024, 4, 128], P('dp', 'sp'), may hold values from -6 to 6
- values: bfloat16 [4, 1024, 4, 128], P('dp', 'sp'), may hold values from -6 to 6
- query_gain: float32 [128], replicated, may hold values from 0.4 to 5
- key_gain: float32 [128], replicated, may hold values from 0.4 to 5
- out_weight: bfloat16 [2048, 2048], P('sp', 'dp'), may hold values from -0.125 to 0.125
- residual: bfloat16 [4, 1024, 2048], P('dp', 'sp'), may hold values from -6 to 6
- norm_gain: float32 [2048], replicated, may hold values from 0.1 to 1.9
- expert_gate: bfloat16 [8, 2048, 1792], P('sp'), may hold values from -0.125 to 0.125
- expert_up: bfloat16 [8, 2048, 1792], P('sp'), may hold values from -0.125 to 0.125
- expert_down: bfloat16 [8, 1792, 2048], P('sp'), may hold values from -0.125 to 0.125
- routes: int32 [4, 1024, 2], P('dp', 'sp'), may hold values from 0 to 7, all different within a row; in each aligned block of 64 rows (0 to 63, 64 to 127, ..., all dimensions but the last counted through in order) at most 32 rows name the same one
- route_weight: float32 [4, 1024, 2], P('dp', 'sp'), may hold values from 0.25 to 1
Outputs:
- layer_out: bfloat16 [4, 1024, 2048], P('dp', 'sp')
The draws below stay inside these ranges and needn't reach their ends.
Inputs may be any that keep to these rules, and one draw needn't show every extreme that they name: `routes`: in each aligned block of 64 rows of one device, no expert is named by more than 32 entries, a bound that some block reaches; the two experts of a row differ.
All inputs are finite; a program needn't handle non-finite values.
Results may differ from the reference program's by a relative error of at most 0.0095.
The reference program's roundings to bfloat16 on the way count: a program that leaves them out, or rounds other values in their place, can miss the bound.
Values may be sent and summed in bfloat16 or wider, within the bound.
A program may use at most 128 MiB of HBM per device.

```python
import math
import jax
import jax.numpy as jnp
import numpy as np
from jax import lax

D = 2048
HEADS = 16
KV_HEADS = 4
HEAD_DIM = 128
EXPERT_FF = 1792
GRID_W = 64
SEQS = 4
LENGTH = 1024
EXPERTS = 8
HALF = 64
CAP = 32


def shared_keys(key):
    drawn = jax.random.normal(jax.random.fold_in(key, 11), (SEQS, LENGTH, KV_HEADS, HEAD_DIM), jnp.float32)
    return jnp.clip(drawn, -6.0, 6.0)


def draw_key_rows(key, part):
    return shared_keys(key).astype(jnp.bfloat16)


def draw_queries(key, part):
    drawn = jax.random.normal(jax.random.fold_in(key, 12), (SEQS, LENGTH, HEADS, HEAD_DIM), jnp.float32)
    drawn = jnp.clip(drawn, -6.0, 6.0)
    return drawn.astype(jnp.bfloat16)


def gain_draw(key, salt):
    drawn = jax.random.normal(jax.random.fold_in(key, salt), (HEAD_DIM,), jnp.float32)
    return 1.0 + 0.18 * jnp.clip(drawn, -3.0, 3.0)


def draw_query_gain(key, part):
    return gain_draw(key, 21)


def draw_key_gain(key, part):
    return gain_draw(key, 22)


def block_levels(stream_key, extent, pieces, low, top_value):
    def one(dim, parts):
        heights = jax.random.uniform(jax.random.fold_in(jax.random.fold_in(stream_key, 6), dim), (parts,), jnp.float32, low / len(pieces), top_value / len(pieces))
        return jnp.repeat(jnp.exp(heights), extent[dim] // parts).reshape((-1,) + (1,) * (len(extent) - dim - 1))

    level = one(*pieces[0])
    for cut in pieces[1:]:
        level = level * one(*cut)
    return level


def shared_out(rng, own, number, rows, number_of, top, reach, skew):
    sequence = jax.random.permutation(rng, number_of)
    packed, ordinary = portions_of(number_of, rows * top, reach, skew, True), portions_of(number_of, rows * top, reach, skew, False)
    places = jnp.arange(number_of)

    def named(tallies, rotation):
        used = int((tallies > 0).sum())
        fixed = max(1, used // 4)
        passed = fixed + (places - fixed + rotation * (used - fixed)) % max(1, number_of - fixed)
        return jnp.zeros((number_of,), jnp.int32).at[sequence[jnp.where(places < fixed, places, passed)]].set(jnp.asarray(tallies, jnp.int32))

    tallies = jnp.where(number % 4 == 0, named(packed, number // 4), named(ordinary, number - number // 4 - 1))
    mixed = jax.random.permutation(jax.random.fold_in(own, 3), number_of)
    donor, sink = mixed[0:number_of // 2 * 2:2], mixed[1:number_of // 2 * 2:2]
    margin = jnp.minimum(tallies[donor] - 1, reach - tallies[sink]) // 2
    margin = jnp.where((donor == sequence[0]) | (sink == sequence[0]) | (tallies[sink] == 0), 0, jnp.maximum(margin, 0))
    passed = jax.random.randint(jax.random.fold_in(own, 4), (number_of // 2,), 0, 1 << 20) % (margin + 1)
    tallies = tallies.at[donor].add(-passed).at[sink].add(passed)
    items = jnp.searchsorted(jnp.cumsum(tallies), jnp.arange(rows * top), side="right").astype(jnp.int32)
    listing = items.reshape(top, rows).T
    listing = listing[jax.random.permutation(jax.random.fold_in(own, 1), rows)]
    rotation = jax.random.randint(jax.random.fold_in(own, 2), (rows, 1), 0, top)
    return jnp.take_along_axis(listing, (jnp.arange(top)[None, :] + rotation) % top, axis=1)


def portions_of(amount, total, most, slope, full):
    weights = [(1 << 20) // math.isqrt(grade ** slope) + 1 for grade in range(1, amount + 1)]
    largest = most if full else min(most, max(-(-total // amount), total * weights[0] // sum(weights)))
    least = 1 if total - largest >= amount - 1 else 0
    counts, spare = [largest] + [least] * (amount - 1), total - largest - least * (amount - 1)
    while spare > 0:
        movable = [i for i in range(1, amount) if counts[i] < largest] or [i for i in range(1, amount) if counts[i] < most]
        mass, budget = sum([weights[i] for i in movable]), spare
        for i in movable:
            addition = min(most - counts[i], max(1, budget * weights[i] // mass), spare)
            counts[i] = counts[i] + addition
            spare = spare - addition
    return np.array(counts)


def gaussian(own_key, dims, deviation, bound, pieces=(), kind=jnp.bfloat16):
    array = jax.random.normal(own_key, dims, jnp.float32) * deviation
    if len(pieces) > 0:
        array = block_levels(own_key, dims, pieces, -0.22, 0.18) * array
    return jnp.clip(array, min=-bound, max=bound).astype(kind)


def setup_inputs(seed: int = 0) -> dict:
    streams_of = jax.random.split(jax.random.key(seed), 14)
    queries = draw_queries(jax.random.fold_in(streams_of[13], 71), 0)
    key_rows = draw_key_rows(jax.random.fold_in(streams_of[13], 71), 0)
    values = gaussian(streams_of[2], (SEQS, LENGTH, KV_HEADS, HEAD_DIM), 1.0, 6.0, ((0, 4), (1, 8)))
    query_gain = draw_query_gain(jax.random.fold_in(streams_of[13], 71), 0)
    key_gain = draw_key_gain(jax.random.fold_in(streams_of[13], 71), 0)
    out_weight = gaussian(streams_of[5], (HEADS * HEAD_DIM, D), (HEADS * HEAD_DIM) ** -0.5, 0.125, ((0, 8), (1, 4)))
    residual = gaussian(streams_of[6], (SEQS, LENGTH, D), 1.0, 6.0, ((0, 4), (1, 8)))
    norm_gain = jnp.clip(1.0 + 0.18 * jax.random.normal(streams_of[7], (D,), jnp.float32), 0.1, 1.9)
    expert_gate = gaussian(streams_of[8], (EXPERTS, D, EXPERT_FF), D ** -0.5, 0.125, ((0, 8),))
    expert_up = gaussian(streams_of[9], (EXPERTS, D, EXPERT_FF), D ** -0.5, 0.125, ((0, 8),))
    expert_down = gaussian(streams_of[10], (EXPERTS, EXPERT_FF, D), EXPERT_FF ** -0.5, 0.125, ((0, 8),))
    routes_keys = jax.random.split(jax.random.fold_in(streams_of[11], 1), SEQS * LENGTH // HALF)
    routes_turns = jax.random.permutation(jax.random.fold_in(streams_of[11], 3), SEQS * LENGTH // HALF)
    routes = jax.vmap(lambda own, number: shared_out(jax.random.fold_in(streams_of[11], 2), own, number, HALF, EXPERTS, 2, CAP, 2))(routes_keys, routes_turns).reshape((SEQS, LENGTH, 2))
    route_weight = jnp.clip(0.25 + 0.75 * jax.random.uniform(streams_of[12], (SEQS, LENGTH, 2), jnp.float32) ** block_levels(streams_of[12], (SEQS, LENGTH, 2), ((0, 4), (1, 8)), -0.2, 0.2), 0.25, 1.0)
    return {"queries": queries, "key_rows": key_rows, "values": values, "query_gain": query_gain, "key_gain": key_gain, "out_weight": out_weight, "residual": residual, "norm_gain": norm_gain, "expert_gate": expert_gate, "expert_up": expert_up, "expert_down": expert_down, "routes": routes, "route_weight": route_weight}


EPS = 1e-06
THETA = 10000.0

def rotate_half(vector, position):
    half_size = vector.shape[-1] // 2
    inverse = THETA ** (-jnp.arange(half_size, dtype=jnp.float32) / half_size)
    angles = position[:, None] * inverse[None, :]
    cosine = jnp.cos(angles)[:, None, :]
    sine_part = jnp.sin(angles)[:, None, :]
    first_part = vector[..., :half_size]
    second_part = vector[..., half_size:]
    return jnp.concatenate([first_part * cosine - second_part * sine_part, first_part * sine_part + second_part * cosine], axis=-1)

def normalize_rotate(vector, gain, positions):
    as_float = vector.astype(jnp.float32)
    scaled = as_float * lax.rsqrt(lax.optimization_barrier(jnp.mean(as_float * as_float, axis=-1, keepdims=True)) + EPS) * gain
    grid_row = (positions // GRID_W).astype(jnp.float32)
    column = (positions % GRID_W).astype(jnp.float32)
    quarter = scaled.shape[-1] // 2
    turned = jnp.concatenate([rotate_half(scaled[..., :quarter], grid_row), rotate_half(scaled[..., quarter:], column)], axis=-1)
    return turned.astype(jnp.bfloat16)

def softmax_rows(scores):
    row_max = lax.optimization_barrier(jnp.max(scores, axis=-1, keepdims=True))
    exponent = jnp.exp(scores - row_max)
    return (exponent / lax.optimization_barrier(jnp.sum(exponent, axis=-1, keepdims=True))).astype(jnp.bfloat16)

def attend_sequence(rot_query, rot_key, value_rows):
    length = rot_query.shape[0]
    group_size = HEADS // KV_HEADS
    block_size = min(512, length)
    key_float = rot_key.astype(jnp.float32)
    value_float = value_rows.astype(jnp.float32)
    grouped = rot_query.reshape(length // block_size, block_size, KV_HEADS, group_size, HEAD_DIM)

    def one_block(query_block):
        scores = jnp.einsum('qhgd,khd->hgqk', query_block.astype(jnp.float32), key_float) * HEAD_DIM ** (-0.5)
        weights = softmax_rows(scores)
        return jnp.einsum('hgqk,khd->qhgd', weights.astype(jnp.float32), value_float).astype(jnp.bfloat16)
    outputs = lax.map(one_block, grouped)
    return outputs.reshape(length, HEADS * HEAD_DIM)

def reference(queries, key_rows, values, query_gain, key_gain, out_weight, residual, norm_gain, expert_gate, expert_up, expert_down, routes, route_weight):
    positions = jnp.arange(LENGTH, dtype=jnp.int32)

    def one_sequence(inputs):
        query_seq, key_seq, value_seq, residual_seq = inputs
        rot_query = normalize_rotate(query_seq, query_gain, positions)
        rot_key = normalize_rotate(key_seq, key_gain, positions)
        attended = attend_sequence(rot_query, rot_key, value_seq)
        return residual_seq.astype(jnp.float32) + jnp.dot(attended, out_weight, preferred_element_type=jnp.float32)
    mixed_sum = lax.map(one_sequence, (queries, key_rows, values, residual))
    flat_mixed = mixed_sum.reshape(-1, D)
    normed = (flat_mixed * lax.rsqrt(lax.optimization_barrier(jnp.mean(flat_mixed * flat_mixed, axis=-1, keepdims=True)) + EPS) * norm_gain).astype(jnp.bfloat16)
    tokens = flat_mixed.shape[0]
    blocks = tokens // HALF
    chosen = routes.reshape(blocks, HALF * 2)
    onehot = (chosen[..., None] == jnp.arange(EXPERTS, dtype=jnp.int32)).astype(jnp.int32)
    slot_rank = lax.optimization_barrier(jnp.sum(jnp.cumsum(onehot, axis=1) * onehot, axis=-1)) - 1
    slot_index = jnp.arange(blocks, dtype=jnp.int32)[:, None] * CAP + slot_rank
    per_expert = blocks * CAP
    target = (chosen * per_expert + slot_index).reshape(-1).astype(jnp.int32)
    source_row = jnp.repeat(jnp.arange(tokens, dtype=jnp.int32), 2)
    row_table = jnp.full((EXPERTS * per_expert,), tokens, jnp.int32).at[target].set(source_row)
    padded = jnp.concatenate([normed, jnp.zeros((1, D), jnp.bfloat16)], axis=0)

    def one_expert(inputs):
        row_ids, gate_weight, up_weight, down_weight = inputs
        selected = padded[row_ids]
        gate_part = jnp.dot(selected, gate_weight, preferred_element_type=jnp.float32)
        up_part = jnp.dot(selected, up_weight, preferred_element_type=jnp.float32)
        hidden = (jax.nn.silu(gate_part) * up_part).astype(jnp.bfloat16)
        return jnp.dot(hidden, down_weight, preferred_element_type=jnp.float32).astype(jnp.bfloat16)
    outputs = lax.map(one_expert, (row_table.reshape(EXPERTS, per_expert), expert_gate, expert_up, expert_down))
    picked = outputs.reshape(-1, D)[target].astype(jnp.float32).reshape(tokens, 2, D)
    weights = route_weight.reshape(tokens, 2, 1)
    result = flat_mixed + lax.optimization_barrier(jnp.sum(picked * weights, axis=1))
    return result.reshape(SEQS, LENGTH, D).astype(jnp.bfloat16)
```

```python
import functools

import jax
import jax.numpy as jnp
from jax import lax
from jax.experimental import pallas as pl
from jax.experimental.pallas import tpu as pltpu
from jax.sharding import PartitionSpec as P

GRID_W = 64
EPS = 1e-06
THETA = 10000.0
MESH = pl.DeviceIdType.MESH
VMEM = pl.BlockSpec(memory_space=pltpu.VMEM)
ANY = pl.BlockSpec(memory_space=pl.ANY)
F32 = jnp.float32
BF16 = jnp.bfloat16


def rotation_tables(positions, head_width):
    quarter = head_width // 4
    inverse = THETA ** (-jnp.arange(quarter, dtype=F32) / quarter)
    grid_row = (positions // GRID_W).astype(F32)[:, None] * inverse[None, :]
    column = (positions % GRID_W).astype(F32)[:, None] * inverse[None, :]
    angles = jnp.concatenate([grid_row, grid_row, column, column], axis=-1)
    lane = jnp.arange(head_width) % (2 * quarter)
    sign = jnp.where(lane < quarter, -1.0, 1.0).astype(F32)
    return jnp.cos(angles), jnp.sin(angles) * sign[None, :]


def turn(rows, gain, cosine, sine):
    width = rows.shape[-1]
    quarter = width // 4
    a = rows.astype(F32)
    a = a * lax.rsqrt(jnp.mean(a * a, axis=-1, keepdims=True) + EPS) * gain
    lane = lax.broadcasted_iota(jnp.int32, a.shape, 1) % (2 * quarter)
    partner = jnp.where(
        lane < quarter, pltpu.roll(a, width - quarter, 1), pltpu.roll(a, quarter, 1)
    )
    return (a * cosine + partner * sine).astype(BF16)


def slot_choice(routes, slots, per_expert):
    rows = routes.shape[0]
    slot = lax.broadcasted_iota(jnp.int32, (rows, slots), 1)
    expert = slot // per_expert
    first = routes[:, 0:1] == expert
    second = routes[:, 1:2] == expert
    named = jnp.where(first | second, 1.0, 0.0).astype(BF16)
    earlier = lax.broadcasted_iota(jnp.int32, (rows, rows), 1) < lax.broadcasted_iota(
        jnp.int32, (rows, rows), 0
    )
    rank = jnp.dot(
        jnp.where(earlier, 1.0, 0.0).astype(BF16), named, preferred_element_type=F32
    )
    here = rank == (slot % per_expert).astype(F32)
    return (
        jnp.where(first & here, 1.0, 0.0).astype(BF16),
        jnp.where(second & here, 1.0, 0.0).astype(BF16),
    )


def attention_kernel(
    n,
    dp,
    slots,
    q_ref,
    k_ref,
    v_ref,
    qg_ref,
    kg_ref,
    cos_ref,
    sin_ref,
    w_ref,
    res_ref,
    ng_ref,
    routes_ref,
    mixed_ref,
    buf_ref,
    q_rot,
    kv,
    w_full,
    att,
    proj,
    back,
    kv_send,
    kv_recv,
    w_send,
    w_recv,
    y_send,
    y_recv,
    pair_send,
    pair_recv,
    fwd_send,
    fwd_recv,
    back_send,
    back_recv,
):
    me = lax.axis_index("sp")
    mine = lax.axis_index("dp")
    heads, rows, width = q_ref.shape
    kv_heads = k_ref.shape[0]
    group = heads // kv_heads
    model = heads * width
    ny = dp // 2
    core = mine % 2
    row_y = mine // 2
    partner = row_y * 2 + 1 - core

    barrier = pltpu.get_barrier_semaphore()
    for d in range(1, n):
        pl.semaphore_signal(
            barrier, inc=1, device_id={"sp": lax.rem(me + d, n)}, device_id_type=MESH
        )
    for d in range(1, dp):
        pl.semaphore_signal(
            barrier, inc=1, device_id={"dp": lax.rem(mine + d, dp)}, device_id_type=MESH
        )

    cosine = cos_ref[...]
    sine = sin_ref[...]
    my_rows = pl.ds(pl.multiple_of(me * rows, rows), rows)
    for g in range(kv_heads):
        kv[g, my_rows, :] = turn(k_ref[g], kg_ref[...], cosine, sine)
        kv[kv_heads + g, my_rows, :] = v_ref[g]
    pl.semaphore_wait(barrier, n - 1 + dp - 1)

    kv_copies = []
    w_rows = w_ref.shape[0]
    my_w = pl.ds(pl.multiple_of(me * w_rows, w_rows), w_rows)
    w_copies = []
    for d in range(1, n):
        copy = pltpu.make_async_remote_copy(
            src_ref=kv.at[:, my_rows, :],
            dst_ref=kv.at[:, my_rows, :],
            send_sem=kv_send.at[d],
            recv_sem=kv_recv.at[d],
            device_id={"sp": lax.rem(me + d, n)},
            device_id_type=MESH,
        )
        copy.start()
        kv_copies.append(copy)
    for d in range(1, n):
        copy = pltpu.make_async_remote_copy(
            src_ref=w_ref,
            dst_ref=w_full.at[my_w],
            send_sem=w_send.at[d],
            recv_sem=w_recv.at[d],
            device_id={"sp": lax.rem(me + d, n)},
            device_id_type=MESH,
        )
        copy.start()
        w_copies.append(copy)
    w_full[my_w] = w_ref[...]

    def turn_head(h, carry):
        q_rot[h] = turn(q_ref[h], qg_ref[...], cosine, sine)
        return carry

    lax.fori_loop(0, heads, turn_head, 0)
    for copy in kv_copies:
        copy.wait()

    per_step = 2
    scale = width ** (-0.5)
    pair_copies = []
    y_copies = {}
    for g in range(kv_heads):

        def some_heads(i, carry):
            first = g * group + i * per_step
            query = q_rot[pl.ds(first, per_step)].reshape(per_step * rows, width)
            scores = (
                lax.dot_general(
                    query, kv[g], (((1,), (1,)), ((), ())), preferred_element_type=F32
                )
                * scale
            )
            exponent = jnp.exp(scores - jnp.max(scores, axis=-1, keepdims=True))
            weights = (exponent / jnp.sum(exponent, axis=-1, keepdims=True)).astype(BF16)
            out = jnp.dot(weights, kv[kv_heads + g], preferred_element_type=F32).astype(BF16)
            for j in range(per_step):
                cols = pl.ds(pl.multiple_of((first + j) * width, width), width)
                att[mine, :, cols] = out[j * rows : (j + 1) * rows]
            return carry

        lax.fori_loop(0, group // per_step, some_heads, 0)
        cols = slice(g * group * width, (g + 1) * group * width)
        for j in range(1, ny):
            copy = pltpu.make_async_remote_copy(
                src_ref=att.at[mine, :, cols],
                dst_ref=att.at[mine, :, cols],
                send_sem=y_send.at[j, g],
                recv_sem=y_recv.at[j, g],
                device_id={"dp": lax.rem(row_y + j, ny) * 2 + core},
                device_id_type=MESH,
            )
            copy.start()
            y_copies[j, g] = copy
        copy = pltpu.make_async_remote_copy(
            src_ref=att.at[mine, :, cols],
            dst_ref=att.at[mine, :, cols],
            send_sem=pair_send.at[g],
            recv_sem=pair_recv.at[g],
            device_id={"dp": partner},
            device_id_type=MESH,
        )
        copy.start()
        pair_copies.append(copy)

    fwd_copies = {}

    def forward(j):
        source = lax.rem(row_y + ny - j, ny) * 2 + core
        for g in range(kv_heads):
            cols = slice(g * group * width, (g + 1) * group * width)
            y_copies[j, g].wait_recv()
            copy = pltpu.make_async_remote_copy(
                src_ref=att.at[source, :, cols],
                dst_ref=att.at[source, :, cols],
                send_sem=fwd_send.at[j, g],
                recv_sem=fwd_recv.at[j, g],
                device_id={"dp": partner},
                device_id_type=MESH,
            )
            copy.start()
            fwd_copies[j, g] = copy
        return source

    for copy in w_copies:
        copy.wait()

    def project(seq):
        return jnp.dot(att[seq], w_full[...], preferred_element_type=F32).astype(BF16)

    back_copies = []

    def send_back(seq, index):
        proj[index] = project(seq)
        copy = pltpu.make_async_remote_copy(
            src_ref=proj.at[index],
            dst_ref=back.at[mine],
            send_sem=back_send.at[index],
            recv_sem=back_recv.at[index],
            device_id={"dp": seq},
            device_id_type=MESH,
        )
        copy.start()
        back_copies.append(copy)

    index = 1
    back[mine] = project(mine)
    for copy in pair_copies:
        copy.wait_recv()
    send_back(partner, index)
    index += 1
    for j in range(1, ny):
        source = forward(j)
        send_back(source, index)
        index += 1
        for g in range(kv_heads):
            fwd_copies[j, g].wait_recv()
        send_back(lax.rem(row_y + ny - j, ny) * 2 + 1 - core, index)
        index += 1

    first_choice, second_choice = slot_choice(routes_ref[...], slots, slots // n)
    choice = first_choice + second_choice
    for copy in pair_copies:
        copy.wait_send()
    for j in range(1, ny):
        for g in range(kv_heads):
            y_copies[j, g].wait_send()
            fwd_copies[j, g].wait_send()
    for copy in back_copies:
        copy.wait()
    block = w_ref.shape[1]
    square = jnp.zeros((rows, 1), F32)
    for s in range(dp):
        cols = slice(s * block, (s + 1) * block)
        part = res_ref[:, cols].astype(F32) + back[s].astype(F32)
        mixed_ref[:, cols] = part
        square = square + jnp.sum(part * part, axis=-1, keepdims=True)
    factor = lax.rsqrt(square / model + EPS)
    for s in range(dp):
        cols = slice(s * block, (s + 1) * block)
        normed = (mixed_ref[:, cols] * factor * ng_ref[:, cols]).astype(BF16)
        buf_ref[:, cols] = lax.dot_general(
            choice, normed, (((0,), (0,)), ((), ())), preferred_element_type=F32
        ).astype(BF16)


def expert_kernel(
    n,
    groups,
    buf_ref,
    gate_hbm,
    up_hbm,
    down_hbm,
    mixed_ref,
    routes_ref,
    rw_ref,
    out_ref,
    gate,
    up,
    down,
    recv,
    hidden,
    res,
    ret,
    load_sem,
    go_send,
    go_recv,
    ret_send,
    ret_recv,
):
    me = lax.axis_index("sp")
    slots, model = buf_ref.shape
    per = slots // n
    ff = gate.shape[1]
    loads = [
        pltpu.make_async_copy(src.at[0], dst, load_sem.at[i])
        for i, (src, dst) in enumerate(((gate_hbm, gate), (up_hbm, up), (down_hbm, down)))
    ]
    barrier = pltpu.get_barrier_semaphore()
    for d in range(1, n):
        pl.semaphore_signal(
            barrier, inc=1, device_id={"sp": lax.rem(me + d, n)}, device_id_type=MESH
        )
    for load in loads:
        load.start()
    pl.semaphore_wait(barrier, n - 1)

    def rows_of(block):
        return pl.ds(pl.multiple_of(block * per, per), per)

    go = [None]
    for d in range(1, n):
        target = lax.rem(me + d, n)
        copy = pltpu.make_async_remote_copy(
            src_ref=buf_ref.at[rows_of(target)],
            dst_ref=recv.at[pl.ds(d * per, per)],
            send_sem=go_send.at[d],
            recv_sem=go_recv.at[d],
            device_id={"sp": target},
            device_id_type=MESH,
        )
        copy.start()
        go.append(copy)
    recv[0:per] = buf_ref[rows_of(me)]
    first_choice, second_choice = slot_choice(routes_ref[...], slots, per)

    share = n // groups
    tile = 256
    back = [None]
    for c in range(groups):
        for d in range(c * share, (c + 1) * share):
            if d > 0:
                go[d].wait_recv()
        lines = slice(c * share * per, (c + 1) * share * per)
        if c == 0:
            loads[0].wait()
            loads[1].wait()

        def up_tile(t, carry):
            cols = pl.ds(pl.multiple_of(t * tile, tile), tile)
            x = recv[lines]
            gate_part = jnp.dot(x, gate[:, cols], preferred_element_type=F32)
            up_part = jnp.dot(x, up[:, cols], preferred_element_type=F32)
            hidden[:, cols] = (gate_part / (1.0 + jnp.exp(-gate_part)) * up_part).astype(BF16)
            return carry

        lax.fori_loop(0, ff // tile, up_tile, 0)
        if c == 0:
            loads[2].wait()

        def down_tile(t, carry):
            cols = pl.ds(pl.multiple_of(t * tile, tile), tile)
            res[lines, cols] = jnp.dot(
                hidden[...], down[:, cols], preferred_element_type=F32
            ).astype(BF16)
            return carry

        lax.fori_loop(0, model // tile, down_tile, 0)
        for d in range(c * share, (c + 1) * share):
            if d == 0:
                ret[rows_of(me)] = res[0:per]
                continue
            copy = pltpu.make_async_remote_copy(
                src_ref=res.at[pl.ds(d * per, per)],
                dst_ref=ret.at[rows_of(me)],
                send_sem=ret_send.at[d],
                recv_sem=ret_recv.at[d],
                device_id={"sp": lax.rem(me + n - d, n)},
                device_id_type=MESH,
            )
            copy.start()
            back.append(copy)
    for d in range(1, n):
        go[d].wait_send()
        back[d].wait()
    for t in range(model // 512):
        cols = slice(t * 512, (t + 1) * 512)
        table = ret[:, cols]
        first = jnp.dot(first_choice, table, preferred_element_type=F32)
        second = jnp.dot(second_choice, table, preferred_element_type=F32)
        out_ref[:, cols] = (
            mixed_ref[:, cols] + (first * rw_ref[:, 0:1] + second * rw_ref[:, 1:2])
        ).astype(BF16)


def on_device(
    n,
    dp,
    queries,
    key_rows,
    values,
    query_gain,
    key_gain,
    out_weight,
    residual,
    norm_gain,
    expert_gate,
    expert_up,
    expert_down,
    routes,
    route_weight,
):
    _, rows, heads, width = queries.shape
    kv_heads = key_rows.shape[2]
    model = heads * width
    length = rows * n
    experts = expert_gate.shape[0] * n
    slots = experts * 2 * max(2, 4 * (rows // 2) // experts)
    positions = lax.axis_index("sp") * rows + jnp.arange(rows, dtype=jnp.int32)
    cosine, sine = rotation_tables(positions, width)
    w_rows, w_cols = out_weight.shape
    dma = pltpu.SemaphoreType.DMA
    ny = dp // 2
    mixed, buffer = pl.pallas_call(
        functools.partial(attention_kernel, n, dp, slots),
        out_shape=(
            jax.ShapeDtypeStruct((rows, model), F32),
            jax.ShapeDtypeStruct((slots, model), BF16),
        ),
        in_specs=[VMEM] * 11,
        out_specs=(VMEM, VMEM),
        scratch_shapes=[
            pltpu.VMEM((heads, rows, width), BF16),
            pltpu.VMEM((2 * kv_heads, length, width), BF16),
            pltpu.VMEM((w_rows * n, w_cols), BF16),
            pltpu.VMEM((dp, rows, model), BF16),
            pltpu.VMEM((dp, rows, w_cols), BF16),
            pltpu.VMEM((dp, rows, w_cols), BF16),
            dma((n,)),
            dma((n,)),
            dma((n,)),
            dma((n,)),
            dma((ny, kv_heads)),
            dma((ny, kv_heads)),
            dma((kv_heads,)),
            dma((kv_heads,)),
            dma((ny, kv_heads)),
            dma((ny, kv_heads)),
            dma((dp,)),
            dma((dp,)),
        ],
        compiler_params=pltpu.CompilerParams(
            collective_id=0, has_side_effects=True, vmem_limit_bytes=40 * 1024 * 1024
        ),
        name="attention",
    )(
        queries[0].transpose(1, 0, 2),
        key_rows[0].transpose(1, 0, 2),
        values[0].transpose(1, 0, 2),
        query_gain[None],
        key_gain[None],
        cosine,
        sine,
        out_weight,
        residual[0],
        norm_gain[None],
        routes[0],
    )
    ff = expert_gate.shape[2]
    groups = 2
    result = pl.pallas_call(
        functools.partial(expert_kernel, n, groups),
        out_shape=jax.ShapeDtypeStruct((rows, model), BF16),
        in_specs=[VMEM, ANY, ANY, ANY, VMEM, VMEM, VMEM],
        out_specs=VMEM,
        scratch_shapes=[
            pltpu.VMEM((model, ff), BF16),
            pltpu.VMEM((model, ff), BF16),
            pltpu.VMEM((ff, model), BF16),
            pltpu.VMEM((slots, model), BF16),
            pltpu.VMEM((slots // groups, ff), BF16),
            pltpu.VMEM((slots, model), BF16),
            pltpu.VMEM((slots, model), BF16),
            dma((3,)),
            dma((n,)),
            dma((n,)),
            dma((n,)),
            dma((n,)),
        ],
        compiler_params=pltpu.CompilerParams(
            collective_id=1, has_side_effects=True, vmem_limit_bytes=56 * 1024 * 1024
        ),
        name="experts",
    )(
        buffer,
        expert_gate,
        expert_up,
        expert_down,
        mixed,
        routes[0],
        route_weight[0],
    )
    return result[None]


def solution(mesh):
    in_specs = (
        P("dp", "sp", None, None),
        P("dp", "sp", None, None),
        P("dp", "sp", None, None),
        P(),
        P(),
        P("sp", "dp"),
        P("dp", "sp", None),
        P(),
        P("sp", None, None),
        P("sp", None, None),
        P("sp", None, None),
        P("dp", "sp", None),
        P("dp", "sp", None),
    )
    out_specs = P("dp", "sp", None)
    return jax.shard_map(
        functools.partial(on_device, mesh.shape["sp"], mesh.shape["dp"]),
        mesh=mesh,
        in_specs=in_specs,
        out_specs=out_specs,
        check_vma=False,
    )
```

```python
import functools

import jax
import jax.numpy as jnp
from jax import lax
from jax.experimental import pallas as pl
from jax.experimental.pallas import tpu as pltpu
from jax.sharding import PartitionSpec as P

GRID_W = 64
EPS = 1e-06
THETA = 10000.0
MESH = pl.DeviceIdType.MESH
VMEM = pl.BlockSpec(memory_space=pltpu.VMEM)
ANY = pl.BlockSpec(memory_space=pl.ANY)
F32 = jnp.float32
BF16 = jnp.bfloat16


def rotation_tables(positions, head_width):
    quarter = head_width // 4
    inverse = THETA ** (-jnp.arange(quarter, dtype=F32) / quarter)
    grid_row = (positions // GRID_W).astype(F32)[:, None] * inverse[None, :]
    column = (positions % GRID_W).astype(F32)[:, None] * inverse[None, :]
    angles = jnp.concatenate([grid_row, grid_row, column, column], axis=-1)
    lane = jnp.arange(head_width) % (2 * quarter)
    sign = jnp.where(lane < quarter, -1.0, 1.0).astype(F32)
    return jnp.cos(angles), jnp.sin(angles) * sign[None, :]


def turn(rows, gain, cosine, sine):
    width = rows.shape[-1]
    quarter = width // 4
    a = rows.astype(F32)
    a = a * lax.rsqrt(jnp.mean(a * a, axis=-1, keepdims=True) + EPS) * gain
    lane = lax.broadcasted_iota(jnp.int32, a.shape, 1) % (2 * quarter)
    partner = jnp.where(
        lane < quarter, pltpu.roll(a, width - quarter, 1), pltpu.roll(a, quarter, 1)
    )
    return (a * cosine + partner * sine).astype(BF16)


class Spread:
    def __init__(self, n, block, send, recv, z_first):
        self.width = max(x for x in range(1, n + 1) if n % x == 0 and x * x <= n)
        self.depth = n // self.width
        self.block, self.send, self.recv, self.z_first = block, send, recv, z_first
        me = lax.axis_index("sp")
        self.z, self.x = me // self.width, me % self.width
        self.ends = []

    def copy(self, source, way, target):
        return pltpu.make_async_remote_copy(
            src_ref=self.block(source),
            dst_ref=self.block(source),
            send_sem=self.send.at[source, way],
            recv_sem=self.recv.at[source],
            device_id={"sp": target},
            device_id_type=MESH,
        )

    def at(self, z, x):
        return z * self.width + x

    def start(self, condition, source, way, target):
        @pl.when(condition)
        def _():
            self.copy(source, way, target).start()

        self.ends.append((condition, source, way, target))

    def up(self, condition, source):
        ok = condition & (self.z < self.depth - 1)
        self.start(ok, source, 0, self.at(self.z + 1, self.x))

    def down(self, condition, source):
        ok = condition & (self.z > 0)
        self.start(ok, source, 1, self.at(self.z - 1, self.x))

    def across(self, condition, source):
        for k in range(1, self.width):
            self.start(condition, source, 1 + k, self.at(self.z, (self.x + k) % self.width))

    def arrive(self, condition, source):
        @pl.when(condition)
        def _():
            self.copy(source, 0, source).wait_recv()

    def columns(self):
        if self.z_first:
            return [self.x]
        return [(self.x + k) % self.width for k in range(self.width)]

    def begin(self):
        own = self.at(self.z, self.x)
        always = self.z >= 0
        if not self.z_first:
            self.across(always, own)
        self.up(always, own)
        self.down(always, own)
        if self.z_first:
            self.across(always, own)

    def second(self):
        always = self.z >= 0
        for x in self.columns()[1:]:
            source = self.at(self.z, x)
            self.arrive(always, source)
            self.up(always, source)
            self.down(always, source)

    def step(self, t):
        for x in self.columns():
            below, above = self.z - t >= 0, self.z + t < self.depth
            source = self.at(self.z - t, x)
            self.arrive(below, source)
            self.up(below, source)
            if self.z_first:
                self.across(below, source)
            source = self.at(self.z + t, x)
            self.arrive(above, source)
            self.down(above, source)
            if self.z_first:
                self.across(above, source)

    def finish(self):
        always = self.z >= 0
        for z in range(self.depth):
            for k in range(1, self.width):
                self.arrive(always, self.at(z, (self.x + k) % self.width))

    def drain(self):
        for condition, source, way, target in self.ends:

            @pl.when(condition)
            def _():
                self.copy(source, way, target).wait_send()


def slot_choice(table, base, slots, capacity):
    rows = table.shape[0]
    slot = lax.broadcasted_iota(jnp.int32, (rows, slots), 1)
    expert = (slot // capacity + base).astype(F32)
    first = table[:, 0:1] == expert
    second = table[:, 1:2] == expert
    named = jnp.where(first | second, 1.0, 0.0).astype(BF16)
    earlier = lax.broadcasted_iota(jnp.int32, (rows, rows), 1) < lax.broadcasted_iota(
        jnp.int32, (rows, rows), 0
    )
    rank = jnp.dot(
        jnp.where(earlier, 1.0, 0.0).astype(BF16), named, preferred_element_type=F32
    )
    here = rank == (slot % capacity).astype(F32)
    return (
        jnp.where(first & here, 1.0, 0.0).astype(BF16),
        jnp.where(second & here, 1.0, 0.0).astype(BF16),
    )


def attention_kernel(
    n,
    dp,
    q_ref,
    k_ref,
    v_ref,
    qg_ref,
    kg_ref,
    cos_ref,
    sin_ref,
    w_ref,
    res_ref,
    ng_ref,
    table_ref,
    mixed_ref,
    normed_ref,
    other_ref,
    q_rot,
    kv,
    w_full,
    att,
    proj,
    back,
    table,
    x_send,
    x_recv,
    t_sem,
    y_send,
    y_recv,
    pair_send,
    pair_recv,
    fwd_send,
    fwd_recv,
    back_send,
    back_recv,
):
    me = lax.axis_index("sp")
    mine = lax.axis_index("dp")
    heads, rows, width = q_ref.shape
    kv_heads = k_ref.shape[0]
    group = heads // kv_heads
    model = heads * width
    ny = dp // 2
    core = mine % 2
    row_y = mine // 2
    partner = row_y * 2 + 1 - core

    barrier = pltpu.get_barrier_semaphore()
    for d in range(1, n):
        pl.semaphore_signal(
            barrier, inc=1, device_id={"sp": lax.rem(me + d, n)}, device_id_type=MESH
        )
    for d in range(1, dp):
        pl.semaphore_signal(
            barrier, inc=1, device_id={"dp": lax.rem(mine + d, dp)}, device_id_type=MESH
        )

    cosine = cos_ref[...]
    sine = sin_ref[...]
    my_rows = pl.ds(pl.multiple_of(me * rows, rows), rows)
    for g in range(kv_heads):
        kv[g, my_rows, :] = turn(k_ref[g], kg_ref[...], cosine, sine)
        kv[kv_heads + g, my_rows, :] = v_ref[g]
    pl.semaphore_wait(barrier, n - 1 + dp - 1)

    w_rows = w_ref.shape[0]
    my_w = pl.ds(pl.multiple_of(me * w_rows, w_rows), w_rows)
    w_full[my_w] = w_ref[...]

    def key_block(s):
        return kv.at[pl.ds(0, kv_heads), pl.ds(pl.multiple_of(s * rows, rows), rows), :]

    def value_block(s):
        return kv.at[pl.ds(kv_heads, kv_heads), pl.ds(pl.multiple_of(s * rows, rows), rows), :]

    def weight_block(part):
        size = w_rows // 2
        return lambda s: w_full.at[
            pl.ds(pl.multiple_of(s * w_rows + part * size, size), size)
        ]

    attention_gather = (
        Spread(n, value_block, x_send.at[0], x_recv.at[0], False),
        Spread(n, key_block, x_send.at[1], x_recv.at[1], True),
    )
    weight_gather = (
        Spread(n, weight_block(1), x_send.at[2], x_recv.at[2], False),
        Spread(n, weight_block(0), x_send.at[3], x_recv.at[3], True),
    )
    table_copy = pltpu.make_async_remote_copy(
        src_ref=table_ref,
        dst_ref=table,
        send_sem=t_sem.at[0],
        recv_sem=t_sem.at[1],
        device_id={"sp": lax.rem(me + n // 2, n)},
        device_id_type=MESH,
    )
    table_copy.start()
    for spread in attention_gather:
        spread.begin()

    def turn_head(h, carry):
        q_rot[h] = turn(q_ref[h], qg_ref[...], cosine, sine)
        return carry

    lax.fori_loop(0, heads, turn_head, 0)
    attention_gather[0].second()
    steps = attention_gather[0].depth
    for t in range(1, steps):
        for spread in attention_gather:
            spread.step(t)
    for spread in weight_gather:
        spread.begin()
    attention_gather[1].finish()

    per_step = 2
    scale = width ** (-0.5)
    pair_copies = []
    y_copies = {}
    for g in range(kv_heads):

        def some_heads(i, carry):
            first = g * group + i * per_step
            query = q_rot[pl.ds(first, per_step)].reshape(per_step * rows, width)
            scores = (
                lax.dot_general(
                    query, kv[g], (((1,), (1,)), ((), ())), preferred_element_type=F32
                )
                * scale
            )
            exponent = jnp.exp(scores - jnp.max(scores, axis=-1, keepdims=True))
            weights = (exponent / jnp.sum(exponent, axis=-1, keepdims=True)).astype(BF16)
            out = jnp.dot(weights, kv[kv_heads + g], preferred_element_type=F32).astype(BF16)
            for j in range(per_step):
                cols = pl.ds(pl.multiple_of((first + j) * width, width), width)
                att[mine, :, cols] = out[j * rows : (j + 1) * rows]
            return carry

        lax.fori_loop(0, group // per_step, some_heads, 0)
        cols = slice(g * group * width, (g + 1) * group * width)
        for j in range(1, ny):
            copy = pltpu.make_async_remote_copy(
                src_ref=att.at[mine, :, cols],
                dst_ref=att.at[mine, :, cols],
                send_sem=y_send.at[j, g],
                recv_sem=y_recv.at[j, g],
                device_id={"dp": lax.rem(row_y + j, ny) * 2 + core},
                device_id_type=MESH,
            )
            copy.start()
            y_copies[j, g] = copy
        copy = pltpu.make_async_remote_copy(
            src_ref=att.at[mine, :, cols],
            dst_ref=att.at[mine, :, cols],
            send_sem=pair_send.at[g],
            recv_sem=pair_recv.at[g],
            device_id={"dp": partner},
            device_id_type=MESH,
        )
        copy.start()
        pair_copies.append(copy)
        if g == 0:
            weight_gather[0].second()

    for t in range(1, steps):
        for spread in weight_gather:
            spread.step(t)
    weight_gather[1].finish()
    fwd_copies = {}

    def forward(j):
        source = lax.rem(row_y + ny - j, ny) * 2 + core
        for g in range(kv_heads):
            cols = slice(g * group * width, (g + 1) * group * width)
            y_copies[j, g].wait_recv()
            copy = pltpu.make_async_remote_copy(
                src_ref=att.at[source, :, cols],
                dst_ref=att.at[source, :, cols],
                send_sem=fwd_send.at[j, g],
                recv_sem=fwd_recv.at[j, g],
                device_id={"dp": partner},
                device_id_type=MESH,
            )
            copy.start()
            fwd_copies[j, g] = copy
        return source

    def project(seq):
        return jnp.dot(att[seq], w_full[...], preferred_element_type=F32).astype(BF16)

    back_copies = []

    def send_back(seq, index):
        proj[index] = project(seq)
        copy = pltpu.make_async_remote_copy(
            src_ref=proj.at[index],
            dst_ref=back.at[mine],
            send_sem=back_send.at[index],
            recv_sem=back_recv.at[index],
            device_id={"dp": seq},
            device_id_type=MESH,
        )
        copy.start()
        back_copies.append(copy)

    index = 1
    back[mine] = project(mine)
    for copy in pair_copies:
        copy.wait_recv()
    send_back(partner, index)
    index += 1
    for j in range(1, ny):
        source = forward(j)
        send_back(source, index)
        index += 1
        for g in range(kv_heads):
            fwd_copies[j, g].wait_recv()
        send_back(lax.rem(row_y + ny - j, ny) * 2 + 1 - core, index)
        index += 1

    for spread in attention_gather + weight_gather:
        spread.drain()
    table_copy.wait()
    other_ref[...] = table[...]
    for copy in pair_copies:
        copy.wait_send()
    for j in range(1, ny):
        for g in range(kv_heads):
            y_copies[j, g].wait_send()
            fwd_copies[j, g].wait_send()
    for copy in back_copies:
        copy.wait()
    block = w_ref.shape[1]
    square = jnp.zeros((rows, 1), F32)
    for s in range(dp):
        cols = slice(s * block, (s + 1) * block)
        part = res_ref[:, cols].astype(F32) + back[s].astype(F32)
        mixed_ref[:, cols] = part
        square = square + jnp.sum(part * part, axis=-1, keepdims=True)
    factor = lax.rsqrt(square / model + EPS)
    for s in range(dp):
        cols = slice(s * block, (s + 1) * block)
        normed_ref[:, cols] = (mixed_ref[:, cols] * factor * ng_ref[:, cols]).astype(BF16)


def expert_kernel(
    n,
    capacity,
    normed_ref,
    mixed_ref,
    own_ref,
    other_ref,
    gate_hbm,
    up_hbm,
    down_hbm,
    out_ref,
    gate,
    up,
    down,
    relay,
    sent,
    recv,
    hidden,
    res,
    ret,
    part,
    home,
    hold,
    load_sem,
    relay_sem,
    home_sem,
    go_send,
    go_recv,
    ret_send,
    ret_recv,
):
    me = lax.axis_index("sp")
    half = n // 2
    base = me // half * half
    mine = me % half
    partner = lax.rem(me + half, n)
    rows, model = normed_ref.shape
    few = rows // 2
    slots = half * capacity
    ff = gate.shape[1]
    loads = [
        pltpu.make_async_copy(src.at[0], dst, load_sem.at[i])
        for i, (src, dst) in enumerate(((gate_hbm, gate), (up_hbm, up), (down_hbm, down)))
    ]

    def peer(k):
        return base + lax.rem(mine + k, half)

    barrier = pltpu.get_barrier_semaphore()
    for target in [partner] + [peer(k) for k in range(1, half)]:
        pl.semaphore_signal(barrier, inc=1, device_id={"sp": target}, device_id_type=MESH)
    for load in loads:
        load.start()
    pl.semaphore_wait(barrier, half)

    relays = []
    for b in range(2):
        copy = pltpu.make_async_remote_copy(
            src_ref=normed_ref.at[pl.ds(b * few, few)],
            dst_ref=relay.at[b],
            send_sem=relay_sem.at[0, b],
            recv_sem=relay_sem.at[1, b],
            device_id={"sp": partner},
            device_id_type=MESH,
        )
        copy.start()
        relays.append(copy)

    def block(index):
        return pl.ds(pl.multiple_of(index * capacity, capacity), capacity)

    go, back, homes = {}, {}, []

    def choices(r):
        table = own_ref if r < 2 else other_ref
        return slot_choice(table[(r % 2) * few : (r % 2 + 1) * few], base, slots, capacity)

    def dispatch(r):
        first, second = choices(r)
        choice = first + second
        lines = normed_ref[(r % 2) * few : (r % 2 + 1) * few] if r < 2 else relay[r % 2]
        for t in range(model // 512):
            cols = slice(t * 512, (t + 1) * 512)
            sent[r, :, cols] = lax.dot_general(
                choice, lines[:, cols], (((0,), (0,)), ((), ())), preferred_element_type=F32
            ).astype(BF16)
        recv[r, block(mine)] = sent[r, block(mine)]
        for k in range(1, half):
            copy = pltpu.make_async_remote_copy(
                src_ref=sent.at[r, block(lax.rem(mine + k, half))],
                dst_ref=recv.at[r, block(mine)],
                send_sem=go_send.at[r, k],
                recv_sem=go_recv.at[r, k],
                device_id={"sp": peer(k)},
                device_id_type=MESH,
            )
            copy.start()
            go[r, k] = copy

    tile = 256

    def serve(r):
        for k in range(1, half):
            go[r, k].wait_recv()

        def up_tile(t, carry):
            cols = pl.ds(pl.multiple_of(t * tile, tile), tile)
            gate_part = jnp.dot(recv[r], gate[:, cols], preferred_element_type=F32)
            up_part = jnp.dot(recv[r], up[:, cols], preferred_element_type=F32)
            hidden[:, cols] = (gate_part / (1.0 + jnp.exp(-gate_part)) * up_part).astype(BF16)
            return carry

        lax.fori_loop(0, ff // tile, up_tile, 0)
        if r == 0:
            loads[2].wait()

        def down_tile(t, carry):
            cols = pl.ds(pl.multiple_of(t * tile, tile), tile)
            res[r, :, cols] = jnp.dot(
                hidden[...], down[:, cols], preferred_element_type=F32
            ).astype(BF16)
            return carry

        lax.fori_loop(0, model // tile, down_tile, 0)
        ret[r, block(mine)] = res[r, block(mine)]
        for k in range(1, half):
            copy = pltpu.make_async_remote_copy(
                src_ref=res.at[r, block(lax.rem(mine + k, half))],
                dst_ref=ret.at[r, block(mine)],
                send_sem=ret_send.at[r, k],
                recv_sem=ret_recv.at[r, k],
                device_id={"sp": peer(k)},
                device_id_type=MESH,
            )
            copy.start()
            back[r, k] = copy

    def combine(r, store):
        first, second = choices(r)
        table = own_ref if r < 2 else other_ref
        lines = slice((r % 2) * few, (r % 2 + 1) * few)
        for k in range(1, half):
            back[r, k].wait_recv()
        for t in range(model // 512):
            cols = slice(t * 512, (t + 1) * 512)
            served = ret[r, :, cols]
            store(
                lines,
                cols,
                jnp.dot(first, served, preferred_element_type=F32) * table[lines, 2:3]
                + jnp.dot(second, served, preferred_element_type=F32) * table[lines, 3:4],
            )

    def store_part(lines, cols, value):
        part[lines, cols] = value.astype(BF16)

    def send_home(b):
        combine(2 + b, store_part)
        copy = pltpu.make_async_remote_copy(
            src_ref=part.at[pl.ds(b * few, few)],
            dst_ref=home.at[b],
            send_sem=home_sem.at[0, b],
            recv_sem=home_sem.at[1, b],
            device_id={"sp": partner},
            device_id_type=MESH,
        )
        copy.start()
        homes.append(copy)

    def store_own(lines, cols, value):
        hold[lines, cols] = mixed_ref[lines, cols] + value

    dispatch(0)
    dispatch(1)
    loads[0].wait()
    loads[1].wait()
    serve(0)
    relays[0].wait_recv()
    dispatch(2)
    serve(1)
    relays[1].wait_recv()
    dispatch(3)
    serve(2)
    serve(3)
    send_home(0)
    send_home(1)
    combine(0, store_own)
    combine(1, store_own)
    for b in range(2):
        homes[b].wait_recv()
        lines = slice(b * few, (b + 1) * few)
        out_ref[lines] = (hold[lines] + home[b].astype(F32)).astype(BF16)
    for b in range(2):
        relays[b].wait_send()
        homes[b].wait_send()
    for r in range(4):
        for k in range(1, half):
            go[r, k].wait_send()
            back[r, k].wait_send()


def on_device(
    n,
    dp,
    queries,
    key_rows,
    values,
    query_gain,
    key_gain,
    out_weight,
    residual,
    norm_gain,
    expert_gate,
    expert_up,
    expert_down,
    routes,
    route_weight,
):
    _, rows, heads, width = queries.shape
    kv_heads = key_rows.shape[2]
    model = heads * width
    length = rows * n
    experts = expert_gate.shape[0] * n
    capacity = max(2, 4 * (rows // 2) // experts)
    slots = n // 2 * capacity
    table = jnp.concatenate([routes[0].astype(F32), route_weight[0]], axis=-1)
    table = jnp.pad(table, ((0, 0), (0, width - table.shape[1])))
    x_width = max(x for x in range(1, n + 1) if n % x == 0 and x * x <= n)
    positions = lax.axis_index("sp") * rows + jnp.arange(rows, dtype=jnp.int32)
    cosine, sine = rotation_tables(positions, width)
    w_rows, w_cols = out_weight.shape
    dma = pltpu.SemaphoreType.DMA
    ny = dp // 2
    mixed, normed, other = pl.pallas_call(
        functools.partial(attention_kernel, n, dp),
        out_shape=(
            jax.ShapeDtypeStruct((rows, model), F32),
            jax.ShapeDtypeStruct((rows, model), BF16),
            jax.ShapeDtypeStruct(table.shape, F32),
        ),
        in_specs=[VMEM] * 11,
        out_specs=(VMEM, VMEM, VMEM),
        scratch_shapes=[
            pltpu.VMEM((heads, rows, width), BF16),
            pltpu.VMEM((2 * kv_heads, length, width), BF16),
            pltpu.VMEM((w_rows * n, w_cols), BF16),
            pltpu.VMEM((dp, rows, model), BF16),
            pltpu.VMEM((dp, rows, w_cols), BF16),
            pltpu.VMEM((dp, rows, w_cols), BF16),
            pltpu.VMEM(table.shape, F32),
            dma((4, n, 1 + x_width)),
            dma((4, n)),
            dma((2,)),
            dma((ny, kv_heads)),
            dma((ny, kv_heads)),
            dma((kv_heads,)),
            dma((kv_heads,)),
            dma((ny, kv_heads)),
            dma((ny, kv_heads)),
            dma((dp,)),
            dma((dp,)),
        ],
        compiler_params=pltpu.CompilerParams(
            collective_id=0, has_side_effects=True, vmem_limit_bytes=40 * 1024 * 1024
        ),
        name="attention",
    )(
        queries[0].transpose(1, 0, 2),
        key_rows[0].transpose(1, 0, 2),
        values[0].transpose(1, 0, 2),
        query_gain[None],
        key_gain[None],
        cosine,
        sine,
        out_weight,
        residual[0],
        norm_gain[None],
        table,
    )
    ff = expert_gate.shape[2]
    few = rows // 2
    result = pl.pallas_call(
        functools.partial(expert_kernel, n, capacity),
        out_shape=jax.ShapeDtypeStruct((rows, model), BF16),
        in_specs=[VMEM, VMEM, VMEM, VMEM, ANY, ANY, ANY],
        out_specs=VMEM,
        scratch_shapes=[
            pltpu.VMEM((model, ff), BF16),
            pltpu.VMEM((model, ff), BF16),
            pltpu.VMEM((ff, model), BF16),
            pltpu.VMEM((2, few, model), BF16),
            pltpu.VMEM((4, slots, model), BF16),
            pltpu.VMEM((4, slots, model), BF16),
            pltpu.VMEM((slots, ff), BF16),
            pltpu.VMEM((4, slots, model), BF16),
            pltpu.VMEM((4, slots, model), BF16),
            pltpu.VMEM((rows, model), BF16),
            pltpu.VMEM((2, few, model), BF16),
            pltpu.VMEM((rows, model), F32),
            dma((3,)),
            dma((2, 2)),
            dma((2, 2)),
            dma((4, n)),
            dma((4, n)),
            dma((4, n)),
            dma((4, n)),
        ],
        compiler_params=pltpu.CompilerParams(
            collective_id=1, has_side_effects=True, vmem_limit_bytes=56 * 1024 * 1024
        ),
        name="experts",
    )(normed, mixed, table, other, expert_gate, expert_up, expert_down)
    return result[None]


def solution(mesh):
    in_specs = (
        P("dp", "sp", None, None),
        P("dp", "sp", None, None),
        P("dp", "sp", None, None),
        P(),
        P(),
        P("sp", "dp"),
        P("dp", "sp", None),
        P(),
        P("sp", None, None),
        P("sp", None, None),
        P("sp", None, None),
        P("dp", "sp", None),
        P("dp", "sp", None),
    )
    out_specs = P("dp", "sp", None)
    return jax.shard_map(
        functools.partial(on_device, mesh.shape["sp"], mesh.shape["dp"]),
        mesh=mesh,
        in_specs=in_specs,
        out_specs=out_specs,
        check_vma=False,
    )
```

```python
import functools

import jax
import jax.numpy as jnp
from jax import lax
from jax.experimental import pallas as pl
from jax.experimental.pallas import tpu as pltpu
from jax.sharding import PartitionSpec as P

GRID_W = 64
EPS = 1e-06
THETA = 10000.0
MESH = pl.DeviceIdType.MESH
VMEM = pl.BlockSpec(memory_space=pltpu.VMEM)
ANY = pl.BlockSpec(memory_space=pl.ANY)
F32 = jnp.float32
BF16 = jnp.bfloat16


def rotation_tables(positions, head_width):
    quarter = head_width // 4
    inverse = THETA ** (-jnp.arange(quarter, dtype=F32) / quarter)
    grid_row = (positions // GRID_W).astype(F32)[:, None] * inverse[None, :]
    column = (positions % GRID_W).astype(F32)[:, None] * inverse[None, :]
    angles = jnp.concatenate([grid_row, grid_row, column, column], axis=-1)
    lane = jnp.arange(head_width) % (2 * quarter)
    sign = jnp.where(lane < quarter, -1.0, 1.0).astype(F32)
    return jnp.cos(angles), jnp.sin(angles) * sign[None, :]


def turn(rows, gain, cosine, sine):
    width = rows.shape[-1]
    quarter = width // 4
    a = rows.astype(F32)
    a = a * lax.rsqrt(jnp.mean(a * a, axis=-1, keepdims=True) + EPS) * gain
    lane = lax.broadcasted_iota(jnp.int32, a.shape, 1) % (2 * quarter)
    partner = jnp.where(
        lane < quarter, pltpu.roll(a, width - quarter, 1), pltpu.roll(a, quarter, 1)
    )
    return (a * cosine + partner * sine).astype(BF16)


class Spread:
    def __init__(self, n, block, send, recv, z_first):
        self.width = max(x for x in range(1, n + 1) if n % x == 0 and x * x <= n)
        self.depth = n // self.width
        self.block, self.send, self.recv, self.z_first = block, send, recv, z_first
        me = lax.axis_index("sp")
        self.z, self.x = me // self.width, me % self.width
        self.ends = []

    def copy(self, source, way, target):
        return pltpu.make_async_remote_copy(
            src_ref=self.block(source),
            dst_ref=self.block(source),
            send_sem=self.send.at[source, way],
            recv_sem=self.recv.at[source],
            device_id={"sp": target},
            device_id_type=MESH,
        )

    def at(self, z, x):
        return z * self.width + x

    def start(self, condition, source, way, target):
        @pl.when(condition)
        def _():
            self.copy(source, way, target).start()

        self.ends.append((condition, source, way, target))

    def up(self, condition, source):
        ok = condition & (self.z < self.depth - 1)
        self.start(ok, source, 0, self.at(self.z + 1, self.x))

    def down(self, condition, source):
        ok = condition & (self.z > 0)
        self.start(ok, source, 1, self.at(self.z - 1, self.x))

    def across(self, condition, source):
        for k in range(1, self.width):
            self.start(condition, source, 1 + k, self.at(self.z, (self.x + k) % self.width))

    def arrive(self, condition, source):
        @pl.when(condition)
        def _():
            self.copy(source, 0, source).wait_recv()

    def columns(self):
        if self.z_first:
            return [self.x]
        return [(self.x + k) % self.width for k in range(self.width)]

    def begin(self):
        own = self.at(self.z, self.x)
        always = self.z >= 0
        if not self.z_first:
            self.across(always, own)
        self.up(always, own)
        self.down(always, own)
        if self.z_first:
            self.across(always, own)

    def second(self):
        always = self.z >= 0
        for x in self.columns()[1:]:
            source = self.at(self.z, x)
            self.arrive(always, source)
            self.up(always, source)
            self.down(always, source)

    def step(self, t):
        for x in self.columns():
            below, above = self.z - t >= 0, self.z + t < self.depth
            source = self.at(self.z - t, x)
            self.arrive(below, source)
            self.up(below, source)
            if self.z_first:
                self.across(below, source)
            source = self.at(self.z + t, x)
            self.arrive(above, source)
            self.down(above, source)
            if self.z_first:
                self.across(above, source)

    def finish(self):
        always = self.z >= 0
        for z in range(self.depth):
            for k in range(1, self.width):
                self.arrive(always, self.at(z, (self.x + k) % self.width))

    def drain(self):
        for condition, source, way, target in self.ends:

            @pl.when(condition)
            def _():
                self.copy(source, way, target).wait_send()


def slot_choice(table, base, slots, capacity):
    rows = table.shape[0]
    slot = lax.broadcasted_iota(jnp.int32, (rows, slots), 1)
    expert = (slot // capacity + base).astype(F32)
    first = table[:, 0:1] == expert
    second = table[:, 1:2] == expert
    named = jnp.where(first | second, 1.0, 0.0).astype(BF16)
    earlier = lax.broadcasted_iota(jnp.int32, (rows, rows), 1) < lax.broadcasted_iota(
        jnp.int32, (rows, rows), 0
    )
    rank = jnp.dot(
        jnp.where(earlier, 1.0, 0.0).astype(BF16), named, preferred_element_type=F32
    )
    here = rank == (slot % capacity).astype(F32)
    return (
        jnp.where(first & here, 1.0, 0.0).astype(BF16),
        jnp.where(second & here, 1.0, 0.0).astype(BF16),
    )


def attention_part(
    n,
    dp,
    start_loads,
    q_ref,
    k_ref,
    v_ref,
    qg_ref,
    kg_ref,
    cos_ref,
    sin_ref,
    w_ref,
    res_ref,
    ng_ref,
    table_ref,
    mixed_ref,
    normed_ref,
    table,
    q_rot,
    kv,
    w_full,
    att,
    proj,
    back,
    res_in,
    gains,
    norm_in,
    in_sem,
    x_send,
    x_recv,
    t_sem,
    y_send,
    y_recv,
    pair_send,
    pair_recv,
    fwd_send,
    fwd_recv,
    back_send,
    back_recv,
):
    me = lax.axis_index("sp")
    mine = lax.axis_index("dp")
    heads, rows, width = q_ref.shape
    kv_heads = k_ref.shape[0]
    group = heads // kv_heads
    model = heads * width
    ny = dp // 2
    core = mine % 2
    row_y = mine // 2
    partner = row_y * 2 + 1 - core

    w_rows = w_ref.shape[0]
    my_w = pl.ds(pl.multiple_of(me * w_rows, w_rows), w_rows)
    fetches = [
        pltpu.make_async_copy(src, dst, in_sem.at[i])
        for i, (src, dst) in enumerate(
            (
                (kg_ref, gains.at[0]),
                (qg_ref, gains.at[1]),
                (w_ref, w_full.at[my_w]),
                (res_ref, res_in),
                (ng_ref, norm_in),
            )
        )
    ]
    for fetch in fetches:
        fetch.start()
    barrier = pltpu.get_barrier_semaphore()
    for d in range(1, n):
        pl.semaphore_signal(
            barrier, inc=1, device_id={"sp": lax.rem(me + d, n)}, device_id_type=MESH
        )
    for d in range(1, dp):
        pl.semaphore_signal(
            barrier, inc=1, device_id={"dp": lax.rem(mine + d, dp)}, device_id_type=MESH
        )

    cosine = cos_ref[...]
    sine = sin_ref[...]
    my_rows = pl.ds(pl.multiple_of(me * rows, rows), rows)
    fetches[0].wait()
    for g in range(kv_heads):
        kv[g, my_rows, :] = turn(k_ref[g], gains[0], cosine, sine)
        kv[kv_heads + g, my_rows, :] = v_ref[g]
    pl.semaphore_wait(barrier, n - 1 + dp - 1)

    def key_block(s):
        return kv.at[pl.ds(0, kv_heads), pl.ds(pl.multiple_of(s * rows, rows), rows), :]

    def value_block(s):
        return kv.at[pl.ds(kv_heads, kv_heads), pl.ds(pl.multiple_of(s * rows, rows), rows), :]

    def weight_block(part):
        size = w_rows // 2
        return lambda s: w_full.at[
            pl.ds(pl.multiple_of(s * w_rows + part * size, size), size)
        ]

    attention_gather = (
        Spread(n, value_block, x_send.at[0], x_recv.at[0], False),
        Spread(n, key_block, x_send.at[1], x_recv.at[1], True),
    )
    weight_gather = (
        Spread(n, weight_block(1), x_send.at[2], x_recv.at[2], False),
        Spread(n, weight_block(0), x_send.at[3], x_recv.at[3], True),
    )
    table_copy = pltpu.make_async_remote_copy(
        src_ref=table_ref,
        dst_ref=table,
        send_sem=t_sem.at[0],
        recv_sem=t_sem.at[1],
        device_id={"sp": lax.rem(me + n // 2, n)},
        device_id_type=MESH,
    )
    table_copy.start()
    for spread in attention_gather:
        spread.begin()

    start_loads()
    fetches[1].wait()

    def turn_head(h, carry):
        q_rot[h] = turn(q_ref[h], gains[1], cosine, sine)
        return carry

    lax.fori_loop(0, heads, turn_head, 0)
    attention_gather[0].second()
    steps = attention_gather[0].depth
    for t in range(1, steps):
        for spread in attention_gather:
            spread.step(t)
        if t == 1:
            fetches[2].wait()
            for spread in weight_gather:
                spread.begin()
    attention_gather[1].finish()

    per_step = 2
    scale = width ** (-0.5)
    pair_copies = []
    y_copies = {}
    for g in range(kv_heads):

        def some_heads(i, carry):
            first = g * group + i * per_step
            query = q_rot[pl.ds(first, per_step)].reshape(per_step * rows, width)
            scores = (
                lax.dot_general(
                    query, kv[g], (((1,), (1,)), ((), ())), preferred_element_type=F32
                )
                * scale
            )
            exponent = jnp.exp(scores - jnp.max(scores, axis=-1, keepdims=True))
            weights = (exponent / jnp.sum(exponent, axis=-1, keepdims=True)).astype(BF16)
            out = jnp.dot(weights, kv[kv_heads + g], preferred_element_type=F32).astype(BF16)
            for j in range(per_step):
                cols = pl.ds(pl.multiple_of((first + j) * width, width), width)
                att[mine, :, cols] = out[j * rows : (j + 1) * rows]
            return carry

        lax.fori_loop(0, group // per_step, some_heads, 0)
        cols = slice(g * group * width, (g + 1) * group * width)
        for j in range(1, ny):
            copy = pltpu.make_async_remote_copy(
                src_ref=att.at[mine, :, cols],
                dst_ref=att.at[mine, :, cols],
                send_sem=y_send.at[j, g],
                recv_sem=y_recv.at[j, g],
                device_id={"dp": lax.rem(row_y + j, ny) * 2 + core},
                device_id_type=MESH,
            )
            copy.start()
            y_copies[j, g] = copy
        copy = pltpu.make_async_remote_copy(
            src_ref=att.at[mine, :, cols],
            dst_ref=att.at[mine, :, cols],
            send_sem=pair_send.at[g],
            recv_sem=pair_recv.at[g],
            device_id={"dp": partner},
            device_id_type=MESH,
        )
        copy.start()
        pair_copies.append(copy)
        if g == 0:
            weight_gather[0].second()

    for t in range(1, steps):
        for spread in weight_gather:
            spread.step(t)
    weight_gather[1].finish()
    fwd_copies = {}

    def forward(j):
        source = lax.rem(row_y + ny - j, ny) * 2 + core
        for g in range(kv_heads):
            cols = slice(g * group * width, (g + 1) * group * width)
            y_copies[j, g].wait_recv()
            copy = pltpu.make_async_remote_copy(
                src_ref=att.at[source, :, cols],
                dst_ref=att.at[source, :, cols],
                send_sem=fwd_send.at[j, g],
                recv_sem=fwd_recv.at[j, g],
                device_id={"dp": partner},
                device_id_type=MESH,
            )
            copy.start()
            fwd_copies[j, g] = copy
        return source

    def project(seq):
        return jnp.dot(att[seq], w_full[...], preferred_element_type=F32).astype(BF16)

    back_copies = []

    def send_back(seq, index):
        proj[index] = project(seq)
        copy = pltpu.make_async_remote_copy(
            src_ref=proj.at[index],
            dst_ref=back.at[mine],
            send_sem=back_send.at[index],
            recv_sem=back_recv.at[index],
            device_id={"dp": seq},
            device_id_type=MESH,
        )
        copy.start()
        back_copies.append(copy)

    index = 1
    back[mine] = project(mine)
    for copy in pair_copies:
        copy.wait_recv()
    send_back(partner, index)
    index += 1
    for j in range(1, ny):
        source = forward(j)
        send_back(source, index)
        index += 1
        for g in range(kv_heads):
            fwd_copies[j, g].wait_recv()
        send_back(lax.rem(row_y + ny - j, ny) * 2 + 1 - core, index)
        index += 1

    for spread in attention_gather + weight_gather:
        spread.drain()
    table_copy.wait()
    fetches[3].wait()
    fetches[4].wait()
    for copy in pair_copies:
        copy.wait_send()
    for j in range(1, ny):
        for g in range(kv_heads):
            y_copies[j, g].wait_send()
            fwd_copies[j, g].wait_send()
    for copy in back_copies:
        copy.wait()
    block = w_ref.shape[1]
    square = jnp.zeros((rows, 1), F32)
    for s in range(dp):
        cols = slice(s * block, (s + 1) * block)
        part = res_in[:, cols].astype(F32) + back[s].astype(F32)
        mixed_ref[:, cols] = part
        square = square + jnp.sum(part * part, axis=-1, keepdims=True)
    factor = lax.rsqrt(square / model + EPS)
    for s in range(dp):
        cols = slice(s * block, (s + 1) * block)
        normed_ref[:, cols] = (mixed_ref[:, cols] * factor * norm_in[:, cols]).astype(BF16)


def expert_part(
    n,
    capacity,
    normed_ref,
    mixed_ref,
    own_ref,
    other_ref,
    loads,
    out_ref,
    gate,
    up,
    down,
    relay,
    sent,
    recv,
    hidden,
    res,
    ret,
    part,
    home,
    hold,
    relay_sem,
    home_sem,
    go_send,
    go_recv,
    ret_send,
    ret_recv,
):
    me = lax.axis_index("sp")
    half = n // 2
    base = me // half * half
    mine = me % half
    partner = lax.rem(me + half, n)
    rows, model = normed_ref.shape
    few = rows // 2
    slots = half * capacity
    ff = gate.shape[1]

    def peer(k):
        return base + lax.rem(mine + k, half)

    relays = []
    for b in range(2):
        copy = pltpu.make_async_remote_copy(
            src_ref=normed_ref.at[pl.ds(b * few, few)],
            dst_ref=relay.at[b],
            send_sem=relay_sem.at[0, b],
            recv_sem=relay_sem.at[1, b],
            device_id={"sp": partner},
            device_id_type=MESH,
        )
        copy.start()
        relays.append(copy)

    def block(index):
        return pl.ds(pl.multiple_of(index * capacity, capacity), capacity)

    go, back, homes = {}, {}, []

    def choices(r):
        table = own_ref if r < 2 else other_ref
        return slot_choice(table[(r % 2) * few : (r % 2 + 1) * few], base, slots, capacity)

    def dispatch(r):
        first, second = choices(r)
        choice = first + second
        lines = normed_ref[(r % 2) * few : (r % 2 + 1) * few] if r < 2 else relay[r % 2]
        for t in range(model // 512):
            cols = slice(t * 512, (t + 1) * 512)
            sent[r, :, cols] = lax.dot_general(
                choice, lines[:, cols], (((0,), (0,)), ((), ())), preferred_element_type=F32
            ).astype(BF16)
        recv[r, block(mine)] = sent[r, block(mine)]
        for k in range(1, half):
            copy = pltpu.make_async_remote_copy(
                src_ref=sent.at[r, block(lax.rem(mine + k, half))],
                dst_ref=recv.at[r, block(mine)],
                send_sem=go_send.at[r, k],
                recv_sem=go_recv.at[r, k],
                device_id={"sp": peer(k)},
                device_id_type=MESH,
            )
            copy.start()
            go[r, k] = copy

    tile = 256

    def serve(r):
        for k in range(1, half):
            go[r, k].wait_recv()

        def up_tile(t, carry):
            cols = pl.ds(pl.multiple_of(t * tile, tile), tile)
            gate_part = jnp.dot(recv[r], gate[:, cols], preferred_element_type=F32)
            up_part = jnp.dot(recv[r], up[:, cols], preferred_element_type=F32)
            hidden[:, cols] = (gate_part / (1.0 + jnp.exp(-gate_part)) * up_part).astype(BF16)
            return carry

        lax.fori_loop(0, ff // tile, up_tile, 0)
        if r == 0:
            loads[2].wait()

        def down_tile(t, carry):
            cols = pl.ds(pl.multiple_of(t * tile, tile), tile)
            res[r, :, cols] = jnp.dot(
                hidden[...], down[:, cols], preferred_element_type=F32
            ).astype(BF16)
            return carry

        lax.fori_loop(0, model // tile, down_tile, 0)
        ret[r, block(mine)] = res[r, block(mine)]
        for k in range(1, half):
            copy = pltpu.make_async_remote_copy(
                src_ref=res.at[r, block(lax.rem(mine + k, half))],
                dst_ref=ret.at[r, block(mine)],
                send_sem=ret_send.at[r, k],
                recv_sem=ret_recv.at[r, k],
                device_id={"sp": peer(k)},
                device_id_type=MESH,
            )
            copy.start()
            back[r, k] = copy

    def combine(r, store):
        first, second = choices(r)
        table = own_ref if r < 2 else other_ref
        lines = slice((r % 2) * few, (r % 2 + 1) * few)
        for k in range(1, half):
            back[r, k].wait_recv()
        for t in range(model // 512):
            cols = slice(t * 512, (t + 1) * 512)
            served = ret[r, :, cols]
            store(
                lines,
                cols,
                jnp.dot(first, served, preferred_element_type=F32) * table[lines, 2:3]
                + jnp.dot(second, served, preferred_element_type=F32) * table[lines, 3:4],
            )

    def store_part(lines, cols, value):
        part[lines, cols] = value.astype(BF16)

    def send_home(b):
        combine(2 + b, store_part)
        copy = pltpu.make_async_remote_copy(
            src_ref=part.at[pl.ds(b * few, few)],
            dst_ref=home.at[b],
            send_sem=home_sem.at[0, b],
            recv_sem=home_sem.at[1, b],
            device_id={"sp": partner},
            device_id_type=MESH,
        )
        copy.start()
        homes.append(copy)

    def store_own(lines, cols, value):
        hold[lines, cols] = mixed_ref[lines, cols] + value

    dispatch(0)
    dispatch(1)
    loads[0].wait()
    loads[1].wait()
    serve(0)
    relays[0].wait_recv()
    dispatch(2)
    serve(1)
    relays[1].wait_recv()
    dispatch(3)
    serve(2)
    serve(3)
    send_home(0)
    send_home(1)
    combine(0, store_own)
    combine(1, store_own)
    for b in range(2):
        homes[b].wait_recv()
        lines = slice(b * few, (b + 1) * few)
        out_ref[lines] = (hold[lines] + home[b].astype(F32)).astype(BF16)
    for b in range(2):
        relays[b].wait_send()
        homes[b].wait_send()
    for r in range(4):
        for k in range(1, half):
            go[r, k].wait_send()
            back[r, k].wait_send()


def layer_kernel(n, dp, capacity, *refs):
    inputs, refs = refs[:11], refs[11:]
    weights, out_ref, refs = refs[:3], refs[3], refs[4:]
    middle, refs = refs[:3], refs[3:]
    attention, refs = refs[:21], refs[21:]
    load_sem, stores, experts = refs[0], refs[1:4], refs[4:]
    loads = [
        pltpu.make_async_copy(src.at[0], dst, load_sem.at[i])
        for i, (src, dst) in enumerate(zip(weights, stores))
    ]

    def start_loads():
        for load in loads:
            load.start()

    attention_part(n, dp, start_loads, *inputs, *middle, *attention)
    mixed, normed, other = middle
    expert_part(n, capacity, normed, mixed, inputs[10], other, loads, out_ref, *stores, *experts)


def on_device(
    n,
    dp,
    queries,
    key_rows,
    values,
    query_gain,
    key_gain,
    out_weight,
    residual,
    norm_gain,
    expert_gate,
    expert_up,
    expert_down,
    routes,
    route_weight,
):
    _, rows, heads, width = queries.shape
    kv_heads = key_rows.shape[2]
    model = heads * width
    length = rows * n
    experts = expert_gate.shape[0] * n
    capacity = max(2, 4 * (rows // 2) // experts)
    slots = n // 2 * capacity
    table = jnp.concatenate([routes[0].astype(F32), route_weight[0]], axis=-1)
    table = jnp.pad(table, ((0, 0), (0, width - table.shape[1])))
    x_width = max(x for x in range(1, n + 1) if n % x == 0 and x * x <= n)
    positions = lax.axis_index("sp") * rows + jnp.arange(rows, dtype=jnp.int32)
    cosine, sine = rotation_tables(positions, width)
    w_rows, w_cols = out_weight.shape
    dma = pltpu.SemaphoreType.DMA
    ny = dp // 2
    ff = expert_gate.shape[2]
    few = rows // 2
    attention_scratch = [
        pltpu.VMEM((heads, rows, width), BF16),
        pltpu.VMEM((2 * kv_heads, length, width), BF16),
        pltpu.VMEM((w_rows * n, w_cols), BF16),
        pltpu.VMEM((dp, rows, model), BF16),
        pltpu.VMEM((dp, rows, w_cols), BF16),
        pltpu.VMEM((dp, rows, w_cols), BF16),
        pltpu.VMEM((rows, model), BF16),
        pltpu.VMEM((2, 1, width), F32),
        pltpu.VMEM((1, model), F32),
        dma((5,)),
        dma((4, n, 1 + x_width)),
        dma((4, n)),
        dma((2,)),
        dma((ny, kv_heads)),
        dma((ny, kv_heads)),
        dma((kv_heads,)),
        dma((kv_heads,)),
        dma((ny, kv_heads)),
        dma((ny, kv_heads)),
        dma((dp,)),
        dma((dp,)),
    ]
    result = pl.pallas_call(
        functools.partial(layer_kernel, n, dp, capacity),
        out_shape=jax.ShapeDtypeStruct((rows, model), BF16),
        in_specs=[VMEM, VMEM, VMEM, ANY, ANY, VMEM, VMEM, ANY, ANY, ANY, VMEM] + [ANY] * 3,
        out_specs=VMEM,
        scratch_shapes=[
            pltpu.VMEM((rows, model), F32),
            pltpu.VMEM((rows, model), BF16),
            pltpu.VMEM(table.shape, F32),
            *attention_scratch,
            dma((3,)),
            pltpu.VMEM((model, ff), BF16),
            pltpu.VMEM((model, ff), BF16),
            pltpu.VMEM((ff, model), BF16),
            pltpu.VMEM((2, few, model), BF16),
            pltpu.VMEM((4, slots, model), BF16),
            pltpu.VMEM((4, slots, model), BF16),
            pltpu.VMEM((slots, ff), BF16),
            pltpu.VMEM((4, slots, model), BF16),
            pltpu.VMEM((4, slots, model), BF16),
            pltpu.VMEM((rows, model), BF16),
            pltpu.VMEM((2, few, model), BF16),
            pltpu.VMEM((rows, model), F32),
            dma((2, 2)),
            dma((2, 2)),
            dma((4, n)),
            dma((4, n)),
            dma((4, n)),
            dma((4, n)),
        ],
        compiler_params=pltpu.CompilerParams(
            collective_id=0, has_side_effects=True, vmem_limit_bytes=56 * 1024 * 1024
        ),
        name="layer",
    )(
        queries[0].transpose(1, 0, 2),
        key_rows[0].transpose(1, 0, 2),
        values[0].transpose(1, 0, 2),
        query_gain[None],
        key_gain[None],
        cosine,
        sine,
        out_weight,
        residual[0],
        norm_gain[None],
        table,
        expert_gate,
        expert_up,
        expert_down,
    )
    return result[None]


def solution(mesh):
    in_specs = (
        P("dp", "sp", None, None),
        P("dp", "sp", None, None),
        P("dp", "sp", None, None),
        P(),
        P(),
        P("sp", "dp"),
        P("dp", "sp", None),
        P(),
        P("sp", None, None),
        P("sp", None, None),
        P("sp", None, None),
        P("dp", "sp", None),
        P("dp", "sp", None),
    )
    out_specs = P("dp", "sp", None)
    return jax.shard_map(
        functools.partial(on_device, mesh.shape["sp"], mesh.shape["dp"]),
        mesh=mesh,
        in_specs=in_specs,
        out_specs=out_specs,
        check_vma=False,
    )
```

```python
import functools

import jax
import jax.numpy as jnp
from jax import lax
from jax.experimental import pallas as pl
from jax.experimental.pallas import tpu as pltpu
from jax.sharding import PartitionSpec as P

GRID_W = 64
EPS = 1e-06
THETA = 10000.0
MESH = pl.DeviceIdType.MESH
VMEM = pl.BlockSpec(memory_space=pltpu.VMEM)
ANY = pl.BlockSpec(memory_space=pl.ANY)
F32 = jnp.float32
BF16 = jnp.bfloat16


def rotation_tables(positions, head_width):
    quarter = head_width // 4
    inverse = THETA ** (-jnp.arange(quarter, dtype=F32) / quarter)
    grid_row = (positions // GRID_W).astype(F32)[:, None] * inverse[None, :]
    column = (positions % GRID_W).astype(F32)[:, None] * inverse[None, :]
    angles = jnp.concatenate([grid_row, grid_row, column, column], axis=-1)
    lane = jnp.arange(head_width) % (2 * quarter)
    sign = jnp.where(lane < quarter, -1.0, 1.0).astype(F32)
    return jnp.cos(angles), jnp.sin(angles) * sign[None, :]


def turn(rows, gain, cosine, sine):
    width = rows.shape[-1]
    quarter = width // 4
    a = rows.astype(F32)
    a = a * lax.rsqrt(jnp.mean(a * a, axis=-1, keepdims=True) + EPS) * gain
    lane = lax.broadcasted_iota(jnp.int32, a.shape, 1) % (2 * quarter)
    partner = jnp.where(
        lane < quarter, pltpu.roll(a, width - quarter, 1), pltpu.roll(a, quarter, 1)
    )
    return (a * cosine + partner * sine).astype(BF16)


class Spread:
    def __init__(self, n, block, send, recv, z_first):
        self.width = max(x for x in range(1, n + 1) if n % x == 0 and x * x <= n)
        self.depth = n // self.width
        self.block, self.send, self.recv, self.z_first = block, send, recv, z_first
        me = lax.axis_index("sp")
        self.z, self.x = me // self.width, me % self.width
        self.ends = []

    def copy(self, source, way, target):
        return pltpu.make_async_remote_copy(
            src_ref=self.block(source),
            dst_ref=self.block(source),
            send_sem=self.send.at[source, way],
            recv_sem=self.recv.at[source],
            device_id={"sp": target},
            device_id_type=MESH,
        )

    def at(self, z, x):
        return z * self.width + x

    def start(self, condition, source, way, target):
        @pl.when(condition)
        def _():
            self.copy(source, way, target).start()

        self.ends.append((condition, source, way, target))

    def up(self, condition, source):
        ok = condition & (self.z < self.depth - 1)
        self.start(ok, source, 0, self.at(self.z + 1, self.x))

    def down(self, condition, source):
        ok = condition & (self.z > 0)
        self.start(ok, source, 1, self.at(self.z - 1, self.x))

    def across(self, condition, source):
        for k in range(1, self.width):
            self.start(condition, source, 1 + k, self.at(self.z, (self.x + k) % self.width))

    def arrive(self, condition, source):
        @pl.when(condition)
        def _():
            self.copy(source, 0, source).wait_recv()

    def columns(self):
        if self.z_first:
            return [self.x]
        return [(self.x + k) % self.width for k in range(self.width)]

    def begin(self):
        own = self.at(self.z, self.x)
        always = self.z >= 0
        if not self.z_first:
            self.across(always, own)
        self.up(always, own)
        self.down(always, own)
        if self.z_first:
            self.across(always, own)

    def second(self):
        always = self.z >= 0
        for x in self.columns()[1:]:
            source = self.at(self.z, x)
            self.arrive(always, source)
            self.up(always, source)
            self.down(always, source)

    def step(self, t):
        for x in self.columns():
            below, above = self.z - t >= 0, self.z + t < self.depth
            source = self.at(self.z - t, x)
            self.arrive(below, source)
            self.up(below, source)
            if self.z_first:
                self.across(below, source)
            source = self.at(self.z + t, x)
            self.arrive(above, source)
            self.down(above, source)
            if self.z_first:
                self.across(above, source)

    def finish(self):
        always = self.z >= 0
        for z in range(self.depth):
            for k in range(1, self.width):
                self.arrive(always, self.at(z, (self.x + k) % self.width))

    def drain(self):
        for condition, source, way, target in self.ends:

            @pl.when(condition)
            def _():
                self.copy(source, way, target).wait_send()


def slot_choice(table, base, slots, capacity):
    rows = table.shape[0]
    slot = lax.broadcasted_iota(jnp.int32, (rows, slots), 1)
    expert = (slot // capacity + base).astype(F32)
    first = table[:, 0:1] == expert
    second = table[:, 1:2] == expert
    named = jnp.where(first | second, 1.0, 0.0).astype(BF16)
    earlier = lax.broadcasted_iota(jnp.int32, (rows, rows), 1) < lax.broadcasted_iota(
        jnp.int32, (rows, rows), 0
    )
    rank = jnp.dot(
        jnp.where(earlier, 1.0, 0.0).astype(BF16), named, preferred_element_type=F32
    )
    here = rank == (slot % capacity).astype(F32)
    return (
        jnp.where(first & here, 1.0, 0.0).astype(BF16),
        jnp.where(second & here, 1.0, 0.0).astype(BF16),
    )


def attention_part(
    n,
    dp,
    start_loads,
    q_ref,
    k_ref,
    v_ref,
    qg_ref,
    kg_ref,
    cos_ref,
    sin_ref,
    w_ref,
    res_ref,
    ng_ref,
    table_ref,
    mixed_ref,
    normed_ref,
    table,
    q_rot,
    kv,
    w_full,
    att,
    proj,
    back,
    res_in,
    gains,
    norm_in,
    in_sem,
    x_send,
    x_recv,
    t_sem,
    y_send,
    y_recv,
    pair_send,
    pair_recv,
    fwd_send,
    fwd_recv,
    back_send,
    back_recv,
):
    me = lax.axis_index("sp")
    mine = lax.axis_index("dp")
    heads, rows, width = q_ref.shape
    kv_heads = k_ref.shape[0]
    group = heads // kv_heads
    model = heads * width
    ny = dp // 2
    core = mine % 2
    row_y = mine // 2
    partner = row_y * 2 + 1 - core

    w_rows = w_ref.shape[0]
    my_w = pl.ds(pl.multiple_of(me * w_rows, w_rows), w_rows)
    fetches = [
        pltpu.make_async_copy(src, dst, in_sem.at[i])
        for i, (src, dst) in enumerate(
            (
                (kg_ref, gains.at[0]),
                (qg_ref, gains.at[1]),
                (w_ref, w_full.at[my_w]),
                (res_ref, res_in),
                (ng_ref, norm_in),
            )
        )
    ]
    for fetch in fetches:
        fetch.start()
    barrier = pltpu.get_barrier_semaphore()
    for d in range(1, n):
        pl.semaphore_signal(
            barrier, inc=1, device_id={"sp": lax.rem(me + d, n)}, device_id_type=MESH
        )
    for d in range(1, dp):
        pl.semaphore_signal(
            barrier, inc=1, device_id={"dp": lax.rem(mine + d, dp)}, device_id_type=MESH
        )

    cosine = cos_ref[...]
    sine = sin_ref[...]
    my_rows = pl.ds(pl.multiple_of(me * rows, rows), rows)
    fetches[0].wait()
    for g in range(kv_heads):
        kv[g, my_rows, :] = turn(k_ref[g], gains[0], cosine, sine)
        kv[kv_heads + g, my_rows, :] = v_ref[g]
    pl.semaphore_wait(barrier, n - 1 + dp - 1)

    def key_block(s):
        return kv.at[pl.ds(0, kv_heads), pl.ds(pl.multiple_of(s * rows, rows), rows), :]

    def value_block(s):
        return kv.at[pl.ds(kv_heads, kv_heads), pl.ds(pl.multiple_of(s * rows, rows), rows), :]

    def weight_block(part):
        size = w_rows // 2
        return lambda s: w_full.at[
            pl.ds(pl.multiple_of(s * w_rows + part * size, size), size)
        ]

    attention_gather = (
        Spread(n, value_block, x_send.at[0], x_recv.at[0], False),
        Spread(n, key_block, x_send.at[1], x_recv.at[1], True),
    )
    weight_gather = (
        Spread(n, weight_block(1), x_send.at[2], x_recv.at[2], False),
        Spread(n, weight_block(0), x_send.at[3], x_recv.at[3], True),
    )
    table_copy = pltpu.make_async_remote_copy(
        src_ref=table_ref,
        dst_ref=table,
        send_sem=t_sem.at[0],
        recv_sem=t_sem.at[1],
        device_id={"sp": lax.rem(me + n // 2, n)},
        device_id_type=MESH,
    )
    table_copy.start()
    for spread in attention_gather:
        spread.begin()

    start_loads()
    fetches[1].wait()

    def turn_head(h, carry):
        q_rot[h] = turn(q_ref[h], gains[1], cosine, sine)
        return carry

    lax.fori_loop(0, heads, turn_head, 0)
    attention_gather[0].second()
    steps = attention_gather[0].depth
    for t in range(1, steps):
        for spread in attention_gather:
            spread.step(t)
        if t == 1:
            fetches[2].wait()
            for spread in weight_gather:
                spread.begin()
    attention_gather[1].finish()

    per_step = 2
    scale = width ** (-0.5)
    pair_copies = []
    y_copies = {}
    for g in range(kv_heads):

        def some_heads(i, carry):
            first = g * group + i * per_step
            query = q_rot[pl.ds(first, per_step)].reshape(per_step * rows, width)
            scores = (
                lax.dot_general(
                    query, kv[g], (((1,), (1,)), ((), ())), preferred_element_type=F32
                )
                * scale
            )
            exponent = jnp.exp(scores - jnp.max(scores, axis=-1, keepdims=True))
            weights = (exponent / jnp.sum(exponent, axis=-1, keepdims=True)).astype(BF16)
            out = jnp.dot(weights, kv[kv_heads + g], preferred_element_type=F32).astype(BF16)
            for j in range(per_step):
                cols = pl.ds(pl.multiple_of((first + j) * width, width), width)
                att[mine, :, cols] = out[j * rows : (j + 1) * rows]
            return carry

        lax.fori_loop(0, group // per_step, some_heads, 0)
        cols = slice(g * group * width, (g + 1) * group * width)
        for j in range(1, ny):
            copy = pltpu.make_async_remote_copy(
                src_ref=att.at[mine, :, cols],
                dst_ref=att.at[mine, :, cols],
                send_sem=y_send.at[j, g],
                recv_sem=y_recv.at[j, g],
                device_id={"dp": lax.rem(row_y + j, ny) * 2 + core},
                device_id_type=MESH,
            )
            copy.start()
            y_copies[j, g] = copy
        copy = pltpu.make_async_remote_copy(
            src_ref=att.at[mine, :, cols],
            dst_ref=att.at[mine, :, cols],
            send_sem=pair_send.at[g],
            recv_sem=pair_recv.at[g],
            device_id={"dp": partner},
            device_id_type=MESH,
        )
        copy.start()
        pair_copies.append(copy)
        if g == 0:
            weight_gather[0].second()

    for t in range(1, steps):
        for spread in weight_gather:
            spread.step(t)
    weight_gather[1].finish()
    fwd_copies = {}

    def forward(j):
        source = lax.rem(row_y + ny - j, ny) * 2 + core
        for g in range(kv_heads):
            cols = slice(g * group * width, (g + 1) * group * width)
            y_copies[j, g].wait_recv()
            copy = pltpu.make_async_remote_copy(
                src_ref=att.at[source, :, cols],
                dst_ref=att.at[source, :, cols],
                send_sem=fwd_send.at[j, g],
                recv_sem=fwd_recv.at[j, g],
                device_id={"dp": partner},
                device_id_type=MESH,
            )
            copy.start()
            fwd_copies[j, g] = copy
        return source

    def project(seq):
        return jnp.dot(att[seq], w_full[...], preferred_element_type=F32).astype(BF16)

    back_copies = []

    def send_back(seq, index):
        proj[index] = project(seq)
        copy = pltpu.make_async_remote_copy(
            src_ref=proj.at[index],
            dst_ref=back.at[mine],
            send_sem=back_send.at[index],
            recv_sem=back_recv.at[index],
            device_id={"dp": seq},
            device_id_type=MESH,
        )
        copy.start()
        back_copies.append(copy)

    index = 1
    back[mine] = project(mine)
    for copy in pair_copies:
        copy.wait_recv()
    send_back(partner, index)
    index += 1
    for j in range(1, ny):
        source = forward(j)
        send_back(source, index)
        index += 1
        for g in range(kv_heads):
            fwd_copies[j, g].wait_recv()
        send_back(lax.rem(row_y + ny - j, ny) * 2 + 1 - core, index)
        index += 1

    for spread in attention_gather + weight_gather:
        spread.drain()
    table_copy.wait()
    fetches[3].wait()
    fetches[4].wait()
    for copy in pair_copies:
        copy.wait_send()
    for j in range(1, ny):
        for g in range(kv_heads):
            y_copies[j, g].wait_send()
            fwd_copies[j, g].wait_send()
    for copy in back_copies:
        copy.wait()
    block = w_ref.shape[1]
    square = jnp.zeros((rows, 1), F32)
    for s in range(dp):
        cols = slice(s * block, (s + 1) * block)
        part = res_in[:, cols].astype(F32) + back[s].astype(F32)
        mixed_ref[:, cols] = part
        square = square + jnp.sum(part * part, axis=-1, keepdims=True)
    factor = lax.rsqrt(square / model + EPS)
    for s in range(dp):
        cols = slice(s * block, (s + 1) * block)
        normed_ref[:, cols] = (mixed_ref[:, cols] * factor * norm_in[:, cols]).astype(BF16)


def expert_part(
    n,
    capacity,
    normed_ref,
    mixed_ref,
    own_ref,
    other_ref,
    loads,
    out_ref,
    gate,
    up,
    down,
    relay,
    sent,
    recv,
    hidden,
    res,
    ret,
    part,
    home,
    hold,
    relay_sem,
    home_sem,
    go_send,
    go_recv,
    ret_send,
    ret_recv,
):
    me = lax.axis_index("sp")
    half = n // 2
    base = me // half * half
    mine = me % half
    partner = lax.rem(me + half, n)
    rows, model = normed_ref.shape
    few = rows // 2
    slots = half * capacity
    ff = gate.shape[1]

    def peer(k):
        return base + lax.rem(mine + k, half)

    relays = []
    for b in range(2):
        copy = pltpu.make_async_remote_copy(
            src_ref=normed_ref.at[pl.ds(b * few, few)],
            dst_ref=relay.at[b],
            send_sem=relay_sem.at[0, b],
            recv_sem=relay_sem.at[1, b],
            device_id={"sp": partner},
            device_id_type=MESH,
        )
        copy.start()
        relays.append(copy)

    def block(index):
        return pl.ds(pl.multiple_of(index * capacity, capacity), capacity)

    go, back, homes = {}, {}, []

    def choices(r):
        table = own_ref if r < 2 else other_ref
        return slot_choice(table[(r % 2) * few : (r % 2 + 1) * few], base, slots, capacity)

    def dispatch(r):
        first, second = choices(r)
        choice = first + second
        lines = normed_ref[(r % 2) * few : (r % 2 + 1) * few] if r < 2 else relay[r % 2]
        for t in range(model // 512):
            cols = slice(t * 512, (t + 1) * 512)
            sent[r, :, cols] = lax.dot_general(
                choice, lines[:, cols], (((0,), (0,)), ((), ())), preferred_element_type=F32
            ).astype(BF16)
        recv[r, block(mine)] = sent[r, block(mine)]
        for k in range(1, half):
            copy = pltpu.make_async_remote_copy(
                src_ref=sent.at[r, block(lax.rem(mine + k, half))],
                dst_ref=recv.at[r, block(mine)],
                send_sem=go_send.at[r, k],
                recv_sem=go_recv.at[r, k],
                device_id={"sp": peer(k)},
                device_id_type=MESH,
            )
            copy.start()
            go[r, k] = copy

    tile = 256

    def serve(r):
        for k in range(1, half):
            go[r, k].wait_recv()

        def up_tile(t, carry):
            cols = pl.ds(pl.multiple_of(t * tile, tile), tile)
            gate_part = jnp.dot(recv[r], gate[:, cols], preferred_element_type=F32)
            up_part = jnp.dot(recv[r], up[:, cols], preferred_element_type=F32)
            hidden[:, cols] = (gate_part / (1.0 + jnp.exp(-gate_part)) * up_part).astype(BF16)
            return carry

        lax.fori_loop(0, ff // tile, up_tile, 0)
        if r == 0:
            loads[2].wait()

        def down_tile(t, carry):
            cols = pl.ds(pl.multiple_of(t * tile, tile), tile)
            res[r, :, cols] = jnp.dot(
                hidden[...], down[:, cols], preferred_element_type=F32
            ).astype(BF16)
            return carry

        lax.fori_loop(0, model // tile, down_tile, 0)
        ret[r, block(mine)] = res[r, block(mine)]
        for k in range(1, half):
            copy = pltpu.make_async_remote_copy(
                src_ref=res.at[r, block(lax.rem(mine + k, half))],
                dst_ref=ret.at[r, block(mine)],
                send_sem=ret_send.at[r, k],
                recv_sem=ret_recv.at[r, k],
                device_id={"sp": peer(k)},
                device_id_type=MESH,
            )
            copy.start()
            back[r, k] = copy

    def combine(r, store):
        first, second = choices(r)
        table = own_ref if r < 2 else other_ref
        lines = slice((r % 2) * few, (r % 2 + 1) * few)
        for k in range(1, half):
            back[r, k].wait_recv()
        for t in range(model // 512):
            cols = slice(t * 512, (t + 1) * 512)
            served = ret[r, :, cols]
            store(
                lines,
                cols,
                jnp.dot(first, served, preferred_element_type=F32) * table[lines, 2:3]
                + jnp.dot(second, served, preferred_element_type=F32) * table[lines, 3:4],
            )

    def store_part(lines, cols, value):
        part[lines, cols] = value.astype(BF16)

    def send_home(b):
        combine(2 + b, store_part)
        copy = pltpu.make_async_remote_copy(
            src_ref=part.at[pl.ds(b * few, few)],
            dst_ref=home.at[b],
            send_sem=home_sem.at[0, b],
            recv_sem=home_sem.at[1, b],
            device_id={"sp": partner},
            device_id_type=MESH,
        )
        copy.start()
        homes.append(copy)

    def store_own(lines, cols, value):
        hold[lines, cols] = mixed_ref[lines, cols] + value

    dispatch(0)
    loads[0].wait()
    loads[1].wait()
    serve(0)
    relays[0].wait_recv()
    dispatch(2)
    dispatch(1)
    relays[1].wait_recv()
    dispatch(3)
    serve(2)
    serve(3)
    send_home(0)
    serve(1)
    send_home(1)
    combine(0, store_own)
    combine(1, store_own)
    for b in range(2):
        homes[b].wait_recv()
        lines = slice(b * few, (b + 1) * few)
        out_ref[lines] = (hold[lines] + home[b].astype(F32)).astype(BF16)
    for b in range(2):
        relays[b].wait_send()
        homes[b].wait_send()
    for r in range(4):
        for k in range(1, half):
            go[r, k].wait_send()
            back[r, k].wait_send()


def layer_kernel(n, dp, capacity, *refs):
    inputs, refs = refs[:11], refs[11:]
    weights, out_ref, refs = refs[:3], refs[3], refs[4:]
    middle, refs = refs[:3], refs[3:]
    attention, refs = refs[:21], refs[21:]
    load_sem, stores, experts = refs[0], refs[1:4], refs[4:]
    loads = [
        pltpu.make_async_copy(src.at[0], dst, load_sem.at[i])
        for i, (src, dst) in enumerate(zip(weights, stores))
    ]

    def start_loads():
        for load in loads:
            load.start()

    attention_part(n, dp, start_loads, *inputs, *middle, *attention)
    mixed, normed, other = middle
    expert_part(n, capacity, normed, mixed, inputs[10], other, loads, out_ref, *stores, *experts)


def on_device(
    n,
    dp,
    queries,
    key_rows,
    values,
    query_gain,
    key_gain,
    out_weight,
    residual,
    norm_gain,
    expert_gate,
    expert_up,
    expert_down,
    routes,
    route_weight,
):
    _, rows, heads, width = queries.shape
    kv_heads = key_rows.shape[2]
    model = heads * width
    length = rows * n
    experts = expert_gate.shape[0] * n
    capacity = max(2, 4 * (rows // 2) // experts)
    slots = n // 2 * capacity
    table = jnp.concatenate([routes[0].astype(F32), route_weight[0]], axis=-1)
    table = jnp.pad(table, ((0, 0), (0, width - table.shape[1])))
    x_width = max(x for x in range(1, n + 1) if n % x == 0 and x * x <= n)
    positions = lax.axis_index("sp") * rows + jnp.arange(rows, dtype=jnp.int32)
    cosine, sine = rotation_tables(positions, width)
    w_rows, w_cols = out_weight.shape
    dma = pltpu.SemaphoreType.DMA
    ny = dp // 2
    ff = expert_gate.shape[2]
    few = rows // 2
    attention_scratch = [
        pltpu.VMEM((heads, rows, width), BF16),
        pltpu.VMEM((2 * kv_heads, length, width), BF16),
        pltpu.VMEM((w_rows * n, w_cols), BF16),
        pltpu.VMEM((dp, rows, model), BF16),
        pltpu.VMEM((dp, rows, w_cols), BF16),
        pltpu.VMEM((dp, rows, w_cols), BF16),
        pltpu.VMEM((rows, model), BF16),
        pltpu.VMEM((2, 1, width), F32),
        pltpu.VMEM((1, model), F32),
        dma((5,)),
        dma((4, n, 1 + x_width)),
        dma((4, n)),
        dma((2,)),
        dma((ny, kv_heads)),
        dma((ny, kv_heads)),
        dma((kv_heads,)),
        dma((kv_heads,)),
        dma((ny, kv_heads)),
        dma((ny, kv_heads)),
        dma((dp,)),
        dma((dp,)),
    ]
    result = pl.pallas_call(
        functools.partial(layer_kernel, n, dp, capacity),
        out_shape=jax.ShapeDtypeStruct((rows, model), BF16),
        in_specs=[VMEM, VMEM, VMEM, ANY, ANY, VMEM, VMEM, ANY, ANY, ANY, VMEM] + [ANY] * 3,
        out_specs=VMEM,
        scratch_shapes=[
            pltpu.VMEM((rows, model), F32),
            pltpu.VMEM((rows, model), BF16),
            pltpu.VMEM(table.shape, F32),
            *attention_scratch,
            dma((3,)),
            pltpu.VMEM((model, ff), BF16),
            pltpu.VMEM((model, ff), BF16),
            pltpu.VMEM((ff, model), BF16),
            pltpu.VMEM((2, few, model), BF16),
            pltpu.VMEM((4, slots, model), BF16),
            pltpu.VMEM((4, slots, model), BF16),
            pltpu.VMEM((slots, ff), BF16),
            pltpu.VMEM((4, slots, model), BF16),
            pltpu.VMEM((4, slots, model), BF16),
            pltpu.VMEM((rows, model), BF16),
            pltpu.VMEM((2, few, model), BF16),
            pltpu.VMEM((rows, model), F32),
            dma((2, 2)),
            dma((2, 2)),
            dma((4, n)),
            dma((4, n)),
            dma((4, n)),
            dma((4, n)),
        ],
        compiler_params=pltpu.CompilerParams(
            collective_id=0, has_side_effects=True, vmem_limit_bytes=56 * 1024 * 1024
        ),
        name="layer",
    )(
        queries[0].transpose(1, 0, 2),
        key_rows[0].transpose(1, 0, 2),
        values[0].transpose(1, 0, 2),
        query_gain[None],
        key_gain[None],
        cosine,
        sine,
        out_weight,
        residual[0],
        norm_gain[None],
        table,
        expert_gate,
        expert_up,
        expert_down,
    )
    return result[None]


def solution(mesh):
    in_specs = (
        P("dp", "sp", None, None),
        P("dp", "sp", None, None),
        P("dp", "sp", None, None),
        P(),
        P(),
        P("sp", "dp"),
        P("dp", "sp", None),
        P(),
        P("sp", None, None),
        P("sp", None, None),
        P("sp", None, None),
        P("dp", "sp", None),
        P("dp", "sp", None),
    )
    out_specs = P("dp", "sp", None)
    return jax.shard_map(
        functools.partial(on_device, mesh.shape["sp"], mesh.shape["dp"]),
        mesh=mesh,
        in_specs=in_specs,
        out_specs=out_specs,
        check_vma=False,
    )
```
